256 devices in a mesh: grp: 2 (over y), sp: 32 (over z, core), tp: 4 (over x).
Axes of the slice: x: 4, y: 2, z: 16, core: 2. Of those that a mesh axis runs over, the one named last changes fastest.
The devices are a block of a 4x16x16 slice.
Arguments:
- resid_in: bfloat16 [8, 2048, 2048], P(('grp', 'tp'), 'sp'), parts along dimension 0, may hold values from -6 to 6
- query_one: bfloat16 [8, 2048, 1024], P('grp', 'sp', 'tp'), parts along dimension 0, may hold values from -624 to 624
- key_one: bfloat16 [8, 2048, 256], P('grp', 'sp', 'tp'), parts along dimension 0, may hold values from -7.78125 to 7.78125
- query_two: bfloat16 [8, 2048, 1024], P('grp', 'sp', 'tp'), parts along dimension 0, may hold values from -624 to 624
- key_two: bfloat16 [8, 2048, 256], P('grp', 'sp', 'tp'), parts along dimension 0, may hold values from -7.78125 to 7.78125
- value: bfloat16 [8, 2048, 512], P('grp', 'sp', 'tp'), parts along dimension 0, may hold values from -6 to 6
- lam: float32 [32], P('tp'), may hold values from 0.3 to 0.8
- head_gain: float32 [64], replicated, may hold values from 0.1 to 1.9
- doc_ids: int32 [8, 2048], P('grp', 'sp'), parts along dimension 0, may hold values from 0 to 3, never falling along the last dimension, each value on 1 to 1024 neighbouring positions
- out_weight: bfloat16 [2048, 2048], P('tp'), may hold values from -0.125 to 0.125
- norm_gain: float32 [2048], replicated, may hold values from 0.1 to 1.9
- gate_weight: bfloat16 [2048, 5632], P('sp', 'tp'), may hold values from -0.125 to 0.125
- value_weight: bfloat16 [2048, 5632], P('sp', 'tp'), may hold values from -0.125 to 0.125
- conv_gate: float32 [3, 5632], P(None, 'tp'), may hold values from -3.5 to 3.5
- conv_value: float32 [3, 5632], P(None, 'tp'), may hold values from -3.5 to 3.5
- down_weight: bfloat16 [5632, 2048], P('tp', 'sp'), may hold values from -0.078125 to 0.078125
Outputs:
- resid_out: bfloat16 [8, 2048, 2048], P(('grp', 'tp'), 'sp'), parts along dimension 0
The draws below stay inside these ranges and needn't reach their ends.
There are 2 independent parts, one for each index of `grp`. The reference program is written for one: setup_inputs(seed, part) draws one part's arguments, and reference() takes and returns one part's arrays. A program takes and returns all parts, laid end to end along the dimension named above; an argument that names none is the same for every part. Nothing has to cross between parts.
All inputs are finite; a program needn't handle non-finite values.
Results may differ from the reference program's by a relative error of at most 0.014.
Values may be sent and summed in bfloat16 or wider, within the bound.
No kernel may reach another device: no remote copies, remote signals or barrier semaphores. Data moves between devices by JAX's collectives and lax.ppermute only.
A program may use at most 128 MiB of HBM per device.

```python
import math
import jax
import jax.numpy as jnp
import numpy as np
from jax import lax

D = 2048
HEADS = 32
KV_HEADS = 8
QK = 32
HEAD_DIM = 64
FF = 5632
SEQS = 4
SEQ_LEN = 2048
N_TP = 4


def drawn_queries(key):
    base = 1.3 * jax.random.normal(jax.random.fold_in(key, 11), (SEQS, SEQ_LEN, HEADS * QK), jnp.float32)
    base = jnp.clip(base, -7.8, 7.8)
    return base.astype(jnp.bfloat16)


def draw_query_one(key, part):
    return drawn_queries(jax.random.fold_in(key, 1))


def draw_query_two(key, part):
    return drawn_queries(jax.random.fold_in(key, 2))


def block_levels(own_key, shape, cuts, least, largest):
    level = 1.0
    for axis_at, parts in cuts:
        steps = jax.random.uniform(jax.random.fold_in(jax.random.fold_in(own_key, 6), axis_at), (parts,), jnp.float32, least / len(cuts), largest / len(cuts))
        level = level * jnp.repeat(jnp.exp(steps), shape[axis_at] // parts).reshape((-1,) + (1,) * (len(shape) - 1 - axis_at))
    return level


def length_profile(number_of, total, most, lean):
    portions = [(1 << 20) // math.isqrt(rank ** lean) + 1 for rank in range(2, number_of + 1)]
    spare, holding = total - most - (number_of - 1), [1] * (number_of - 1)
    while spare > 0:
        movable = [i for i in range(number_of - 1) if holding[i] < most]
        pool, left = sum([portions[i] for i in movable]), spare
        for i in movable:
            addition = min(most - holding[i], max(1, left * portions[i] // pool), spare)
            holding[i] = holding[i] + addition
            spare = spare - addition
    return np.array([most] + holding)


def ragged(own_key, amount, total, limit, slope):
    if amount == 2:
        one = jax.random.randint(own_key, (), max(1, total - limit), min(limit, total - 1) + 1)
        return jnp.stack([one, total - one])
    lengths = jnp.asarray(length_profile(amount, total, limit, slope), jnp.int32)
    twos = (amount - 1) // 2
    giver, sink = lengths[1:1 + 2 * twos:2], lengths[2:2 + 2 * twos:2]
    margin = jnp.minimum(giver - 1, limit - sink)
    shifted = jax.random.randint(jax.random.fold_in(own_key, 1), (twos,), 0, 1 << 20) % (margin + 1)
    lengths = lengths.at[1:1 + 2 * twos:2].set(giver - shifted).at[2:2 + 2 * twos:2].set(sink + shifted)
    return lengths[jax.random.permutation(jax.random.fold_in(own_key, 2), amount)]


def noise(stream_key, extent, scale, bound, pieces=(), kind=jnp.bfloat16):
    drawn = scale * jax.random.normal(stream_key, extent, jnp.float32)
    if pieces:
        drawn = drawn * block_levels(stream_key, extent, pieces, -0.22, 0.18)
    return jnp.clip(drawn, -bound, bound).astype(kind)


def setup_inputs(seed: int = 0, part: int = 0) -> dict:
    arg_keys = jax.random.split(jax.random.key(seed), 17)
    part_keys = jax.random.split(jax.random.fold_in(arg_keys[16], part), 17)
    resid_in = noise(part_keys[0], (SEQS, SEQ_LEN, D), 1.0, 6.0, ((0, 4), (1, 32)))
    query_one = draw_query_one(jax.random.fold_in(jax.random.fold_in(arg_keys[16], part), 71), part)
    key_one = noise(part_keys[2], (SEQS, SEQ_LEN, KV_HEADS * QK), 1.3, 7.78125, ((1, 32), (2, 4)))
    query_two = draw_query_two(jax.random.fold_in(jax.random.fold_in(arg_keys[16], part), 71), part)
    key_two = noise(part_keys[4], (SEQS, SEQ_LEN, KV_HEADS * QK), 1.3, 7.78125, ((1, 32), (2, 4)))
    value = noise(part_keys[5], (SEQS, SEQ_LEN, KV_HEADS * HEAD_DIM), 1.0, 6.0, ((1, 32), (2, 4)))
    lam = jnp.clip(0.3 + 0.5 * jax.random.uniform(arg_keys[6], (HEADS,), jnp.float32) ** block_levels(arg_keys[6], (HEADS,), ((0, 4),), -0.2, 0.2), 0.3, 0.8)
    head_gain = jnp.clip(1.0 + 0.18 * jax.random.normal(arg_keys[7], (HEAD_DIM,), jnp.float32), 0.1, 1.9)
    doc_ids = jax.vmap(lambda own: jnp.searchsorted(jnp.cumsum(ragged(own, 4, SEQ_LEN, SEQ_LEN // 2, 1)), jnp.arange(SEQ_LEN), side="right"))(jax.random.split(part_keys[8], SEQS)).reshape((SEQS, SEQ_LEN)).astype(jnp.int32)
    out_weight = noise(arg_keys[9], (HEADS * HEAD_DIM, D), (HEADS * HEAD_DIM) ** -0.5, 0.125, ((0, 4),))
    norm_gain = jnp.clip(1.0 + 0.18 * jax.random.normal(arg_keys[10], (D,), jnp.float32), 0.1, 1.9)
    gate_weight = noise(arg_keys[11], (D, FF), D ** -0.5, 0.125, ((0, 32), (1, 4)))
    value_weight = noise(arg_keys[12], (D, FF), D ** -0.5, 0.125, ((0, 32), (1, 4)))
    conv_gate = noise(arg_keys[13], (3, FF), 3 ** -0.5, 3.5, ((1, 4),), jnp.float32)
    conv_value = noise(arg_keys[14], (3, FF), 3 ** -0.5, 3.5, ((1, 4),), jnp.float32)
    down_weight = noise(arg_keys[15], (FF, D), FF ** -0.5, 0.078125, ((0, 4), (1, 32)))
    return dict(resid_in=resid_in, query_one=query_one, key_one=key_one, query_two=query_two, key_two=key_two, value=value, lam=lam, head_gain=head_gain, doc_ids=doc_ids, out_weight=out_weight, norm_gain=norm_gain, gate_weight=gate_weight, value_weight=value_weight, conv_gate=conv_gate, conv_value=conv_value, down_weight=down_weight)


NEG_BIG = -1e+30
NORM_EPS = 1e-06
ROPE_BASE = 500000.0

def rotate(block, positions, heads):
    entries = block.astype(jnp.float32).reshape(block.shape[:-1] + (heads, -1))
    width = entries.shape[-1]
    half = width // 2
    freqs = ROPE_BASE ** (-jnp.arange(half, dtype=jnp.float32) * 2.0 / width)
    angles = positions.astype(jnp.float32)[:, None] * freqs[None, :]
    cosine = jnp.cos(angles)[:, None, :]
    sine = jnp.sin(angles)[:, None, :]
    first = entries[..., :half]
    second = entries[..., half:]
    turned = jnp.concatenate([first * cosine - second * sine, second * cosine + first * sine], axis=-1)
    return turned.astype(jnp.bfloat16)

def depthwise(edge, current, taps, edge_docs, docs):
    count = current.shape[0]
    extended = jnp.concatenate([edge, current], axis=0).astype(jnp.float32)
    ext_docs = jnp.concatenate([edge_docs, docs], axis=0)
    total = taps[2][None, :] * extended[2:]
    for shift_k in range(2):
        same = (ext_docs[shift_k:shift_k + count] == docs)[:, None]
        total = total + jnp.where(same, taps[shift_k][None, :] * extended[shift_k:shift_k + count], 0.0)
    return total

def head_rows(args, positions, docs, gain):
    q_one, k_one, q_two, k_two, vals, weight = args
    tokens = vals.shape[0]
    blk = math.gcd(tokens, 512)
    scale = q_one.shape[-1] ** (-0.5)

    def one_block(index):
        start = index * blk
        qpos = start + jnp.arange(blk, dtype=jnp.int32)
        qdoc = lax.dynamic_slice_in_dim(docs, start, blk, 0)
        allowed = (positions[None, :] <= qpos[:, None]) & (docs[None, :] == qdoc[:, None])

        def branch(q_all, k_all):
            qblock = lax.dynamic_slice_in_dim(q_all, start, blk, 0)
            scores = jnp.dot(qblock, k_all.T, preferred_element_type=jnp.float32) * scale
            scores = jnp.where(allowed, scores, NEG_BIG)
            peak = lax.optimization_barrier(jnp.max(scores, axis=-1, keepdims=True))
            expd = jnp.where(allowed, jnp.exp(scores - peak), 0.0)
            numer = jnp.dot(expd.astype(jnp.bfloat16), vals, preferred_element_type=jnp.float32)
            return numer / lax.optimization_barrier(jnp.sum(expd, axis=-1, keepdims=True))
        mixed = branch(q_one, k_one) - weight * branch(q_two, k_two)
        meansq = lax.optimization_barrier(jnp.mean(mixed * mixed, axis=-1, keepdims=True))
        return (mixed * lax.rsqrt(meansq + NORM_EPS) * gain[None, :]).astype(jnp.bfloat16)
    out = lax.map(one_block, jnp.arange(tokens // blk))
    return out.reshape(tokens, -1)

def grouped_product(left, right, groups):
    width = left.shape[1] // groups
    total = jnp.zeros((left.shape[0], right.shape[1]), jnp.float32)
    for group in range(groups):
        part = jnp.dot(left[:, group * width:(group + 1) * width], right[group * width:(group + 1) * width], preferred_element_type=jnp.float32).astype(jnp.bfloat16)
        part = lax.optimization_barrier(part)
        total = total + part.astype(jnp.float32)
    return total

def reference(resid_in, query_one, key_one, query_two, key_two, value, lam, head_gain, doc_ids, out_weight, norm_gain, gate_weight, value_weight, conv_gate, conv_value, down_weight):
    heads = lam.shape[0]
    key_width = query_one.shape[2] // heads
    kv_heads = key_one.shape[2] // key_width
    group = heads // kv_heads

    def by_head(block):
        return jnp.transpose(block, (1, 0, 2))

    def one_sequence(args):
        resid, q_a, k_a, q_b, k_b, vals_in, docs = args
        tokens = resid.shape[0]
        positions = jnp.arange(tokens, dtype=jnp.int32)
        q_first = by_head(rotate(q_a, positions, heads))
        k_first = jnp.repeat(by_head(rotate(k_a, positions, kv_heads)), group, axis=0)
        q_second = by_head(rotate(q_b, positions, heads))
        k_second = jnp.repeat(by_head(rotate(k_b, positions, kv_heads)), group, axis=0)
        vals = jnp.repeat(by_head(vals_in.reshape(tokens, kv_heads, -1)), group, axis=0)
        per_head = lax.map(lambda items: head_rows(items, positions, docs, head_gain), (q_first, k_first, q_second, k_second, vals, lam))
        heads_out = jnp.transpose(per_head, (1, 0, 2)).reshape(tokens, -1)
        proj = grouped_product(heads_out, out_weight, N_TP)
        mid = resid.astype(jnp.float32) + proj
        meansq = lax.optimization_barrier(jnp.mean(mid * mid, axis=-1, keepdims=True))
        normed = (mid * lax.rsqrt(meansq + NORM_EPS) * norm_gain[None, :]).astype(jnp.bfloat16)
        up_gate = jnp.dot(normed, gate_weight, preferred_element_type=jnp.float32).astype(jnp.bfloat16)
        up_value = jnp.dot(normed, value_weight, preferred_element_type=jnp.float32).astype(jnp.bfloat16)
        edge = jnp.zeros((2, up_gate.shape[1]), jnp.bfloat16)
        edge_docs = jnp.full((2,), -1, jnp.int32)
        conv_g = depthwise(edge, up_gate, conv_gate, edge_docs, docs)
        conv_v = depthwise(edge, up_value, conv_value, edge_docs, docs)
        hidden = (jax.nn.silu(conv_g) * conv_v).astype(jnp.bfloat16)
        down = grouped_product(hidden, down_weight, N_TP)
        return (mid + down).astype(jnp.bfloat16)
    return lax.map(one_sequence, (resid_in, query_one, key_one, query_two, key_two, value, doc_ids))
```

```python
import math

import jax
import jax.numpy as jnp
from jax import lax
from jax.experimental import pallas as pl
from jax.experimental.pallas import tpu as pltpu
from jax.sharding import PartitionSpec as P

NORM_EPS = 1e-06
ROPE_BASE = 500000.0
LOG2E = math.log2(math.e)
DOC_SPAN = 1024
KEY_UP = 4096.0
VAL_UP = 8192.0
LANES = 128
EDGE = 8


def shifted(array, axis, by):
    length = lax.axis_size(axis)
    return lax.ppermute(array, axis, [(i, (i + by) % length) for i in range(length)])


def from_behind(array, axis):
    length = lax.axis_size(axis)
    return lax.ppermute(array, axis, [(i, i + 1) for i in range(length - 1)])


def turn_tables(positions, width):
    half = width // 2
    freqs = ROPE_BASE ** (-jnp.arange(half, dtype=jnp.float32) * 2.0 / width)
    angles = positions.astype(jnp.float32)[:, None] * freqs[None, :]
    cosine = jnp.cos(angles)
    sine = jnp.sin(angles)
    times = LANES // width
    return (
        jnp.tile(jnp.concatenate([cosine, cosine], axis=1), (1, times)),
        jnp.tile(jnp.concatenate([-sine, sine], axis=1), (1, times)),
    )


def attend(q_one, q_two, window, cosine, sine, doc_cols, gain, lam, place):
    seqs, rows, q_lanes = q_one.shape
    ranks, per_rank, _ = window.shape
    keys = ranks * rows
    heads = lam.shape[0]
    width = q_lanes // heads
    half = width // 2
    kv_heads = 2
    group = heads // kv_heads
    head_width = LANES // kv_heads
    mult = width ** (-0.5) * LOG2E

    def body(place_ref, lam_ref, q1_ref, q2_ref, w_ref, c_ref, s_ref, d_ref, g_ref, o_ref):
        first_key = place_ref[0]
        first_row = place_ref[1]
        own = place_ref[2]
        lane = lax.broadcasted_iota(jnp.int32, (rows, LANES), 1)
        low = (lane % width) < half
        cos = c_ref[...]
        sin = s_ref[...]
        gain_row = g_ref[...]
        key_pos = first_key + lax.broadcasted_iota(jnp.int32, (rows, keys), 1)
        row_pos = first_row + lax.broadcasted_iota(jnp.int32, (rows, keys), 0)
        causal = key_pos <= row_pos
        even_lane = lax.broadcasted_iota(jnp.int32, (1, LANES), 1) < rows
        ones = jnp.ones((keys, LANES), jnp.bfloat16)
        for s in range(seqs):
            at = s * rows
            k_all = w_ref[:, at : at + rows, 0:LANES].reshape(keys, LANES)
            v_all = w_ref[:, at : at + rows, LANES : 2 * LANES].reshape(keys, LANES)
            v_ext = jnp.concatenate([v_all, ones], axis=1)
            pieces = []
            for i in range(ranks // 2):
                tail_a = w_ref[2 * i, seqs * rows : per_rank, 0:LANES].astype(jnp.float32)
                tail_b = w_ref[2 * i + 1, seqs * rows : per_rank, 0:LANES].astype(jnp.float32)
                pieces.append(jnp.where(even_lane, tail_a[s : s + 1], tail_b[s : s + 1]))
            key_doc = jnp.concatenate(pieces, axis=1)
            row_doc = d_ref[:, s : s + 1]
            bias = jnp.where(causal & (key_doc == row_doc), 0.0, -1e30)
            placed = []
            for ref in (q1_ref, q2_ref):
                tiles = []
                for h in range(kv_heads):
                    x = ref[s, :, h * LANES : (h + 1) * LANES].astype(jnp.float32)
                    swap = jnp.where(
                        low, pltpu.roll(x, LANES - half, 1), pltpu.roll(x, half, 1)
                    )
                    tiles.append((x * cos + swap * sin).astype(jnp.bfloat16).astype(jnp.float32))
                placed.append(tiles)
            for h in range(kv_heads):
                result = []
                for c in range(2):
                    target = c * kv_heads + h
                    inside = (lane // width) == target
                    parts = []
                    for g in range(group):
                        by = (width * (target - g)) % LANES
                        x = placed[c][h]
                        x = pltpu.roll(x, by, 1) if by else x
                        parts.append(jnp.where(inside, x, 0.0).astype(jnp.bfloat16))
                    q = jnp.concatenate(parts, axis=0)
                    score = lax.dot_general(
                        q, k_all, (((1,), (1,)), ((), ())), preferred_element_type=jnp.float32
                    )
                    score = score.reshape(group, rows, keys) + bias[None]
                    peak = jnp.max(score, axis=-1, keepdims=True)
                    expd = jnp.exp2((score - peak) * mult).astype(jnp.bfloat16)
                    both = jnp.dot(
                        expd.reshape(group * rows, keys), v_ext, preferred_element_type=jnp.float32
                    )
                    result.append(both[:, :LANES] / both[:, LANES:])
                here = (lane // head_width) == h
                outs = []
                for g in range(group):
                    a = result[0][g * rows : (g + 1) * rows]
                    b = result[1][g * rows : (g + 1) * rows]
                    o = jnp.where(here, a - lam_ref[h * group + g] * b, 0.0)
                    meansq = jnp.sum(o * o, axis=-1, keepdims=True) * (1.0 / head_width)
                    o = o * lax.rsqrt(meansq + NORM_EPS) * gain_row
                    if (g % 2) != h:
                        o = pltpu.roll(o, head_width, 1)
                    outs.append(o)
                slot = (s - own + seqs) % seqs
                for j in range(group // 2):
                    tile = (h * group) // 2 + j
                    o_ref[slot, :, tile * LANES : (tile + 1) * LANES] = (
                        outs[2 * j] + outs[2 * j + 1]
                    ).astype(jnp.bfloat16)

    vmem = pl.BlockSpec(memory_space=pltpu.VMEM)
    smem = pl.BlockSpec(memory_space=pltpu.SMEM)
    return pl.pallas_call(
        body,
        out_shape=jax.ShapeDtypeStruct((seqs, rows, heads * head_width), jnp.bfloat16),
        in_specs=[smem, smem] + [vmem] * 7,
        out_specs=vmem,
        name="attend",
    )(place, lam, q_one, q_two, window, cosine, sine, doc_cols, gain)


def feed_forward(blocks, weights, same, conv_gate, conv_value):
    span, width = blocks[0].shape
    count = len(blocks)
    total = span * count
    rows = span - EDGE
    hidden = conv_gate.shape[1]
    step = 2 * LANES
    cuts = [(a, min(a + step, hidden)) for a in range(0, hidden, step)]
    out_step = 4 * LANES

    def body(x0, x1, x2, x3, same_ref, cg_ref, cv_ref, w_hbm, o_ref, x_ref, w_ref, h_ref, sems):
        def up_copy(j):
            a, b = cuts[j]
            return [
                pltpu.make_async_copy(
                    w_hbm.at[:, base + a : base + b],
                    w_ref.at[:, base + a : base + b],
                    sems.at[2 * j + which],
                )
                for which, base in enumerate((0, hidden))
            ]

        down_copy = pltpu.make_async_copy(
            w_hbm.at[:, 2 * hidden : 3 * hidden],
            w_ref.at[:, 2 * hidden : 3 * hidden],
            sems.at[2 * len(cuts)],
        )
        for j in range(len(cuts)):
            for copy in up_copy(j):
                copy.start()
        down_copy.start()
        for k, x in enumerate((x0, x1, x2, x3)):
            x_ref[k * span : (k + 1) * span, :] = x[...]
        one_back = same_ref[:, 0:1]
        two_back = same_ref[:, 1:2]
        for j in range(len(cuts)):
            a, b = cuts[j]
            for copy in up_copy(j):
                copy.wait()
            convs = []
            for base, taps in ((0, cg_ref), (hidden, cv_ref)):
                u = jnp.dot(
                    x_ref[...], w_ref[:, base + a : base + b], preferred_element_type=jnp.float32
                )
                u = u.astype(jnp.bfloat16).astype(jnp.float32)
                convs.append(
                    taps[2:3, a:b] * u
                    + taps[1:2, a:b] * (one_back * pltpu.roll(u, 1, 0))
                    + taps[0:1, a:b] * (two_back * pltpu.roll(u, 2, 0))
                )
            g, v = convs
            act = (g / (1.0 + jnp.exp(-g)) * v).astype(jnp.float32)
            for k in range(count):
                h_ref[k * rows : (k + 1) * rows, a:b] = act[
                    k * span + EDGE : (k + 1) * span
                ].astype(jnp.bfloat16)
        down_copy.wait()
        for a in range(0, width, out_step):
            part = lax.dot_general(
                h_ref[...],
                w_ref[a : a + out_step, 2 * hidden : 3 * hidden],
                (((1,), (1,)), ((), ())),
                preferred_element_type=jnp.float32,
            )
            o_ref[:, :, a : a + out_step] = part.astype(jnp.bfloat16).reshape(count, rows, out_step)

    vmem = pl.BlockSpec(memory_space=pltpu.VMEM)
    return pl.pallas_call(
        body,
        out_shape=jax.ShapeDtypeStruct((count, rows, width), jnp.bfloat16),
        in_specs=[vmem] * 7 + [pl.BlockSpec(memory_space=pltpu.HBM)],
        out_specs=vmem,
        scratch_shapes=[
            pltpu.VMEM((total, width), jnp.bfloat16),
            pltpu.VMEM((width, 3 * hidden), jnp.bfloat16),
            pltpu.VMEM((count * rows, hidden), jnp.bfloat16),
            pltpu.SemaphoreType.DMA((2 * len(cuts) + 1,)),
        ],
        compiler_params=pltpu.CompilerParams(vmem_limit_bytes=56 * 1024 * 1024),
        name="feed_forward",
    )(*blocks, same, conv_gate, conv_value, weights)


def per_device(
    resid_in,
    query_one,
    key_one,
    query_two,
    key_two,
    value,
    lam,
    head_gain,
    doc_ids,
    out_weight,
    norm_gain,
    gate_weight,
    value_weight,
    conv_gate,
    conv_value,
    down_weight,
):
    seqs, rows, q_lanes = query_one.shape
    width = q_lanes // lam.shape[0]
    rank = lax.axis_index("sp")
    ranks = lax.axis_size("sp")
    own = lax.axis_index("tp")
    parts = lax.axis_size("tp")
    model = resid_in.shape[2]

    packed = jnp.concatenate([gate_weight, value_weight, down_weight.T], axis=1)
    weights = lax.all_gather(packed, "sp", axis=0, tiled=True)

    positions = rank * rows + jnp.arange(rows, dtype=jnp.int32)
    cosine, sine = turn_tables(positions, width)
    keys = jnp.concatenate([key_one, key_two], axis=2).astype(jnp.float32)
    half = width // 2
    low = (jnp.arange(LANES) % width) < half
    swap = jnp.where(low, jnp.roll(keys, -half, axis=2), jnp.roll(keys, half, axis=2))
    keys = (keys * cosine + swap * sine).astype(jnp.bfloat16).astype(jnp.float32) * KEY_UP
    vals = value.astype(jnp.float32) * VAL_UP
    body_rows = jnp.concatenate([keys, vals], axis=2).reshape(seqs * rows, 2 * LANES)
    doc_rows = jnp.tile(doc_ids.astype(jnp.float32) * KEY_UP, (1, 2 * LANES // rows))
    doc_rows = jnp.pad(doc_rows, ((0, EDGE - seqs), (0, 0)))
    sent = jnp.concatenate([body_rows, doc_rows], axis=0).astype(jnp.float16)
    everyone = lax.all_gather(sent, "sp", axis=0, tiled=False)

    back = DOC_SPAN // rows
    span = min(back + 2, ranks)
    first = jnp.clip(rank // 2 * 2 - back, 0, ranks - span)
    lanes_down = jnp.where(jnp.arange(2 * LANES) < LANES, 1.0 / KEY_UP, 1.0 / VAL_UP)
    window = lax.dynamic_slice_in_dim(everyone, first, span, 0)
    window = (window.astype(jnp.float32) * lanes_down).astype(jnp.bfloat16)
    behind = lax.dynamic_index_in_dim(everyone, jnp.maximum(rank - 1, 0), 0, keepdims=False)
    behind = behind[seqs * rows : seqs * rows + seqs, rows - 2 : rows].astype(jnp.float32)
    behind = jnp.where(rank > 0, behind * (1.0 / KEY_UP), -1.0)

    docs = doc_ids.astype(jnp.float32)
    gain = jnp.tile(head_gain, 2).reshape(1, LANES)
    place = jnp.stack([first * rows, rank * rows, own]).astype(jnp.int32)
    heads_out = attend(
        query_one, query_two, window, cosine, sine, docs.T, gain, lam, place
    )
    proj = jnp.dot(
        heads_out.reshape(seqs * rows, -1), out_weight, preferred_element_type=jnp.float32
    )
    proj = proj.astype(jnp.bfloat16).reshape(seqs, rows, model)
    mid = resid_in[0].astype(jnp.float32) + proj[0].astype(jnp.float32)
    for k in range(1, parts):
        mid = mid + shifted(proj[k], "tp", k).astype(jnp.float32)
    meansq = jnp.mean(mid * mid, axis=-1, keepdims=True)
    normed = (mid * lax.rsqrt(meansq + NORM_EPS) * norm_gain).astype(jnp.bfloat16)
    edge = from_behind(normed[rows - EDGE :], "sp")
    block = jnp.concatenate([edge, normed], axis=0)
    blocks = [block] + [shifted(block, "tp", k) for k in range(1, parts)]

    joined = jnp.concatenate([behind, docs], axis=1)
    same = jnp.stack([joined[:, 1 : rows + 1] == docs, joined[:, :rows] == docs], axis=-1)
    same = jnp.pad(same.astype(jnp.float32), ((0, 0), (EDGE, 0), (0, 0)))
    order = (own - jnp.arange(parts)) % parts
    pick = (order[:, None] == jnp.arange(seqs)[None, :]).astype(jnp.float32)
    same = jnp.sum(pick[:, :, None, None] * same[None], axis=1)
    partial = feed_forward(
        blocks, weights, same.reshape(parts * (rows + EDGE), 2), conv_gate, conv_value
    )
    out = mid + partial[0].astype(jnp.float32)
    for k in range(1, parts):
        out = out + shifted(partial[k], "tp", -k).astype(jnp.float32)
    return out.astype(jnp.bfloat16)[None]


def solution(mesh):
    placed = (
        P(("grp", "tp"), "sp", None),
        P("grp", "sp", "tp"),
        P("grp", "sp", "tp"),
        P("grp", "sp", "tp"),
        P("grp", "sp", "tp"),
        P("grp", "sp", "tp"),
        P("tp"),
        P(),
        P("grp", "sp"),
        P("tp", None),
        P(),
        P("sp", "tp"),
        P("sp", "tp"),
        P(None, "tp"),
        P(None, "tp"),
        P("tp", "sp"),
    )
    return jax.shard_map(
        per_device,
        mesh=mesh,
        in_specs=placed,
        out_specs=P(("grp", "tp"), "sp", None),
        check_vma=False,
    )
```

```python
import math

import jax
import jax.numpy as jnp
from jax import lax
from jax.experimental import pallas as pl
from jax.experimental.pallas import tpu as pltpu
from jax.sharding import PartitionSpec as P

NORM_EPS = 1e-06
ROPE_BASE = 500000.0
LOG2E = math.log2(math.e)
DOC_SPAN = 1024
KEY_UP = 4096.0
VAL_UP = 8192.0
LANES = 128
EDGE = 8


def shifted(array, axis, by):
    length = lax.axis_size(axis)
    return lax.ppermute(array, axis, [(i, (i + by) % length) for i in range(length)])


def from_behind(array, axis):
    length = lax.axis_size(axis)
    return lax.ppermute(array, axis, [(i, i + 1) for i in range(length - 1)])


def turn_tables(positions, width):
    half = width // 2
    freqs = ROPE_BASE ** (-jnp.arange(half, dtype=jnp.float32) * 2.0 / width)
    angles = positions.astype(jnp.float32)[:, None] * freqs[None, :]
    cosine = jnp.cos(angles)
    sine = jnp.sin(angles)
    times = LANES // width
    return (
        jnp.tile(jnp.concatenate([cosine, cosine], axis=1), (1, times)),
        jnp.tile(jnp.concatenate([-sine, sine], axis=1), (1, times)),
    )


def attend(place, q_one, q_two, window, cosine, sine, docs, gain, lam, out_weight, after):
    seqs, rows, q_lanes = q_one.shape
    ranks, per_rank, _ = window.shape
    keys = ranks * rows
    heads = lam.shape[0]
    width = q_lanes // heads
    half = width // 2
    kv_heads = 2
    group = heads // kv_heads
    head_width = LANES // kv_heads
    mult = width ** (-0.5) * LOG2E
    model = out_weight.shape[1]

    def body(
        place_ref, lam_ref, q1_ref, q2_ref, w_ref, e_ref, c_ref, s_ref, d_ref, g_ref, p_ref, _,
        o_ref, m_ref, h_ref,
    ):
        s = place_ref[0]
        first_key = place_ref[1]
        first_row = place_ref[2]
        lane = lax.broadcasted_iota(jnp.int32, (rows, LANES), 1)
        low = (lane % width) < half
        cos = c_ref[...]
        sin = s_ref[...]
        gain_row = jnp.concatenate([g_ref[...], g_ref[...]], axis=1)
        k_all = w_ref[:, :, 0:LANES].reshape(keys, LANES)
        v_all = w_ref[:, :, LANES : 2 * LANES].reshape(keys, LANES)
        v_ext = jnp.concatenate([v_all, jnp.ones((keys, LANES), jnp.bfloat16)], axis=1)

        placed = []
        for ref in (q1_ref, q2_ref):
            tiles = []
            for h in range(kv_heads):
                x = ref[0, :, h * LANES : (h + 1) * LANES].astype(jnp.float32)
                swap = jnp.where(low, pltpu.roll(x, LANES - half, 1), pltpu.roll(x, half, 1))
                tiles.append((x * cos + swap * sin).astype(jnp.bfloat16).astype(jnp.float32))
            placed.append(tiles)

        def scores(h, c):
            target = c * kv_heads + h
            inside = (lane // width) == target
            parts = []
            for g in range(group):
                by = (width * (target - g)) % LANES
                x = placed[c][h]
                x = pltpu.roll(x, by, 1) if by else x
                parts.append(jnp.where(inside, x, 0.0).astype(jnp.bfloat16))
            q = jnp.concatenate(parts, axis=0)
            return lax.dot_general(
                q, k_all, (((1,), (1,)), ((), ())), preferred_element_type=jnp.float32
            )

        key_pos = first_key + lax.broadcasted_iota(jnp.int32, (rows, keys), 1)
        row_pos = first_row + lax.broadcasted_iota(jnp.int32, (rows, keys), 0)
        even_lane = lax.broadcasted_iota(jnp.int32, (1, LANES), 1) < rows
        this_row = lax.broadcasted_iota(jnp.int32, (EDGE, LANES), 0) == s
        pieces = []
        for i in range(ranks // 2):
            two = [
                jnp.sum(
                    jnp.where(this_row, e_ref[2 * i + b, :, 0:LANES].astype(jnp.float32), 0.0),
                    axis=0,
                    keepdims=True,
                )
                for b in range(2)
            ]
            pieces.append(jnp.where(even_lane, two[0], two[1]))
        key_doc = jnp.concatenate(pieces, axis=1)
        diagonal = lax.broadcasted_iota(jnp.int32, (rows, rows), 0) == lax.broadcasted_iota(
            jnp.int32, (rows, rows), 1
        )
        row_doc = jnp.sum(
            jnp.where(diagonal, d_ref[pl.ds(s, 1), :].astype(jnp.float32), 0.0),
            axis=1,
            keepdims=True,
        )
        equal = key_doc == row_doc
        bias = jnp.where((key_pos <= row_pos) & equal, 0.0, -1e30)
        ones_back = [
            jnp.sum(
                jnp.where(equal & (key_pos == row_pos - by), 1.0, 0.0), axis=1, keepdims=True
            )
            for by in (1, 2)
        ]
        m_ref[...] = jnp.where(lane == 0, ones_back[0], ones_back[1])

        pairs = [(h, c) for h in range(kv_heads) for c in range(2)]
        upcoming = scores(*pairs[0])
        results = []
        for at in range(len(pairs)):
            score = upcoming
            if at + 1 < len(pairs):
                upcoming = scores(*pairs[at + 1])
            score = score.reshape(group, rows, keys) + bias[None]
            peak = jnp.max(score, axis=-1, keepdims=True)
            expd = jnp.exp2((score - peak) * mult).astype(jnp.bfloat16)
            both = jnp.dot(
                expd.reshape(group * rows, keys), v_ext, preferred_element_type=jnp.float32
            )
            results.append(both[:, :LANES] / both[:, LANES:])
        for h in range(kv_heads):
            here = (lane // head_width) == h
            outs = []
            for g in range(group):
                a = results[2 * h][g * rows : (g + 1) * rows]
                b = results[2 * h + 1][g * rows : (g + 1) * rows]
                o = jnp.where(here, a - lam_ref[h * group + g] * b, 0.0)
                meansq = jnp.sum(o * o, axis=-1, keepdims=True) * (1.0 / head_width)
                o = o * lax.rsqrt(meansq + NORM_EPS) * gain_row
                if (g % 2) != h:
                    o = pltpu.roll(o, head_width, 1)
                outs.append(o)
            for j in range(group // 2):
                tile = (h * group) // 2 + j
                h_ref[:, tile * LANES : (tile + 1) * LANES] = (
                    outs[2 * j] + outs[2 * j + 1]
                ).astype(jnp.bfloat16)
        o_ref[...] = jnp.dot(
            h_ref[...], p_ref[...], preferred_element_type=jnp.float32
        ).astype(jnp.bfloat16)

    whole = lambda *shape: pl.BlockSpec(shape, lambda i, p: (0,) * len(shape))
    smem = pl.BlockSpec(memory_space=pltpu.SMEM)
    return pl.pallas_call(
        body,
        out_shape=(
            jax.ShapeDtypeStruct((rows, model), jnp.bfloat16),
            jax.ShapeDtypeStruct((rows, LANES), jnp.float32),
        ),
        grid_spec=pltpu.PrefetchScalarGridSpec(
            num_scalar_prefetch=1,
            grid=(1,),
            in_specs=[
                smem,
                pl.BlockSpec((1, rows, q_lanes), lambda i, p: (p[0], 0, 0)),
                pl.BlockSpec((1, rows, q_lanes), lambda i, p: (p[0], 0, 0)),
                pl.BlockSpec((ranks, rows, 2 * LANES), lambda i, p: (0, p[0], 0)),
                pl.BlockSpec((ranks, EDGE, 2 * LANES), lambda i, p: (0, seqs * rows // EDGE, 0)),
                whole(rows, LANES),
                whole(rows, LANES),
                whole(seqs, rows),
                whole(1, head_width),
                whole(*out_weight.shape),
                pl.BlockSpec(memory_space=pl.ANY),
            ],
            out_specs=(whole(rows, model), whole(rows, LANES)),
            scratch_shapes=[pltpu.VMEM((rows, heads * head_width), jnp.bfloat16)],
        ),
        cost_estimate=pl.CostEstimate(flops=3_000_000_000, transcendentals=0, bytes_accessed=4_000_000),
        name="attend",
    )(place, lam, q_one, q_two, window, window, cosine, sine, docs, gain, out_weight, after)


def feed_forward(blocks, edges, same, weights, conv_gate, conv_value):
    rows, width = blocks[0].shape
    count = len(blocks)
    span = rows + EDGE
    total = span * count
    hidden = conv_gate.shape[1]
    step = 2 * LANES
    cuts = [(a, min(a + step, hidden)) for a in range(0, hidden, step)]
    out_step = 4 * LANES

    def body(*refs):
        x_in, e_in, m_in = refs[:count], refs[count : 2 * count], refs[2 * count : 3 * count]
        cg_ref, cv_ref, w_hbm = refs[3 * count : 3 * count + 3]
        outs = refs[3 * count + 3 : 4 * count + 3]
        x_ref, w_ref, h_ref, b_ref, sems = refs[4 * count + 3 :]

        def piece(base, a, b, at):
            return pltpu.make_async_copy(
                w_hbm.at[:, base + a : base + b], w_ref.at[:, base + a : base + b], sems.at[at]
            )

        ups = [
            [piece(base, a, b, 2 * j + n) for n, base in enumerate((0, hidden))]
            for j, (a, b) in enumerate(cuts)
        ]
        down = piece(2 * hidden, 0, hidden, 2 * len(cuts))
        for both in ups:
            for copy in both:
                copy.start()
        down.start()
        for k in range(count):
            x_ref[k * span : k * span + EDGE, :] = e_in[k][...]
            x_ref[k * span + EDGE : (k + 1) * span, :] = x_in[k][...]
            b_ref[k * span : k * span + EDGE, :] = jnp.zeros((EDGE, LANES), jnp.float32)
            b_ref[k * span + EDGE : (k + 1) * span, :] = m_in[k][...]
        one_back = b_ref[:, 0:1]
        two_back = b_ref[:, 1:2]

        def raised(j):
            a, b = cuts[j]
            for copy in ups[j]:
                copy.wait()
            return [
                jnp.dot(
                    x_ref[...], w_ref[:, base + a : base + b], preferred_element_type=jnp.float32
                ).astype(jnp.bfloat16)
                for base in (0, hidden)
            ]

        upcoming = raised(0)
        for j in range(len(cuts)):
            a, b = cuts[j]
            current = upcoming
            if j + 1 < len(cuts):
                upcoming = raised(j + 1)
            convs = []
            for u, taps in zip(current, (cg_ref, cv_ref)):
                u = u.astype(jnp.float32)
                convs.append(
                    taps[2:3, a:b] * u
                    + taps[1:2, a:b] * (one_back * pltpu.roll(u, 1, 0))
                    + taps[0:1, a:b] * (two_back * pltpu.roll(u, 2, 0))
                )
            g, v = convs
            act = g / (1.0 + jnp.exp(-g)) * v
            for k in range(count):
                h_ref[k * rows : (k + 1) * rows, a:b] = act[
                    k * span + EDGE : (k + 1) * span
                ].astype(jnp.bfloat16)
        down.wait()
        for a in range(0, width, out_step):
            part = lax.dot_general(
                h_ref[...],
                w_ref[a : a + out_step, 2 * hidden : 3 * hidden],
                (((1,), (1,)), ((), ())),
                preferred_element_type=jnp.float32,
            ).astype(jnp.bfloat16)
            for k in range(count):
                outs[k][:, a : a + out_step] = part[k * rows : (k + 1) * rows]

    vmem = pl.BlockSpec(memory_space=pltpu.VMEM)
    return pl.pallas_call(
        body,
        out_shape=[jax.ShapeDtypeStruct((rows, width), jnp.bfloat16)] * count,
        in_specs=[vmem] * (3 * count + 2) + [pl.BlockSpec(memory_space=pltpu.HBM)],
        out_specs=[vmem] * count,
        scratch_shapes=[
            pltpu.VMEM((total, width), jnp.bfloat16),
            pltpu.VMEM((width, 3 * hidden), jnp.bfloat16),
            pltpu.VMEM((count * rows, hidden), jnp.bfloat16),
            pltpu.VMEM((total, LANES), jnp.float32),
            pltpu.SemaphoreType.DMA((2 * len(cuts) + 1,)),
        ],
        compiler_params=pltpu.CompilerParams(vmem_limit_bytes=56 * 1024 * 1024),
        name="feed_forward",
    )(*blocks, *edges, *same, conv_gate, conv_value, weights)


def per_device(
    resid_in,
    query_one,
    key_one,
    query_two,
    key_two,
    value,
    lam,
    head_gain,
    doc_ids,
    out_weight,
    norm_gain,
    gate_weight,
    value_weight,
    conv_gate,
    conv_value,
    down_weight,
):
    seqs, rows, q_lanes = query_one.shape
    width = q_lanes // lam.shape[0]
    rank = lax.axis_index("sp")
    ranks = lax.axis_size("sp")
    own = lax.axis_index("tp")
    parts = lax.axis_size("tp")
    model = resid_in.shape[2]

    packed = jnp.concatenate([gate_weight, value_weight, down_weight.T], axis=1)
    weights = lax.all_gather(packed, "sp", axis=0, tiled=True)

    positions = rank * rows + jnp.arange(rows, dtype=jnp.int32)
    cosine, sine = turn_tables(positions, width)
    keys = jnp.concatenate([key_one, key_two], axis=2).astype(jnp.float32)
    half = width // 2
    low = (jnp.arange(LANES) % width) < half
    swap = jnp.where(low, jnp.roll(keys, -half, axis=2), jnp.roll(keys, half, axis=2))
    keys = (keys * cosine + swap * sine).astype(jnp.bfloat16).astype(jnp.float32) * KEY_UP
    vals = value.astype(jnp.float32) * VAL_UP
    body_rows = jnp.concatenate([keys, vals], axis=2).reshape(seqs * rows, 2 * LANES)
    doc_rows = jnp.tile(doc_ids.astype(jnp.float32) * KEY_UP, (1, 2 * LANES // rows))
    doc_rows = jnp.pad(doc_rows, ((0, EDGE - seqs), (0, 0)))
    sent = jnp.concatenate([body_rows, doc_rows], axis=0).astype(jnp.float16)
    everyone = lax.all_gather(sent, "sp", axis=0, tiled=False)

    back = DOC_SPAN // rows
    span = min(back + 2, ranks)
    first = jnp.clip(rank // 2 * 2 - back, 0, ranks - span)
    lanes_down = jnp.where(jnp.arange(2 * LANES) < LANES, 1.0 / KEY_UP, 1.0 / VAL_UP)
    window = lax.dynamic_slice_in_dim(everyone, first, span, 0)
    window = (window.astype(jnp.float32) * lanes_down).astype(jnp.bfloat16)
    gain = head_gain.reshape(1, -1)
    proj = [None] * parts
    same = [None] * parts
    after = lam
    farthest_first = sorted(range(parts), key=lambda k: -min(k, parts - k))
    for k in farthest_first:
        place = jnp.stack([(own + k) % parts, first * rows, rank * rows]).astype(jnp.int32)
        proj[k], same[-k] = attend(
            place, query_one, query_two, window, cosine, sine, doc_ids, gain, lam, out_weight, after
        )
        after = proj[k]
    mid = resid_in[0].astype(jnp.float32) + proj[0].astype(jnp.float32)
    for k in range(1, parts):
        mid = mid + shifted(proj[k], "tp", k).astype(jnp.float32)
    meansq = jnp.mean(mid * mid, axis=-1, keepdims=True)
    normed = (mid * lax.rsqrt(meansq + NORM_EPS) * norm_gain).astype(jnp.bfloat16)
    edge = from_behind(normed[rows - EDGE :], "sp")
    blocks = [normed] + [shifted(normed, "tp", k) for k in range(1, parts)]
    edges = [edge] + [shifted(edge, "tp", k) for k in range(1, parts)]
    partial = feed_forward(blocks, edges, same, weights, conv_gate, conv_value)
    out = mid + partial[0].astype(jnp.float32)
    for k in range(1, parts):
        out = out + shifted(partial[k], "tp", -k).astype(jnp.float32)
    return out.astype(jnp.bfloat16)[None]


def solution(mesh):
    placed = (
        P(("grp", "tp"), "sp", None),
        P("grp", "sp", "tp"),
        P("grp", "sp", "tp"),
        P("grp", "sp", "tp"),
        P("grp", "sp", "tp"),
        P("grp", "sp", "tp"),
        P("tp"),
        P(),
        P("grp", "sp"),
        P("tp", None),
        P(),
        P("sp", "tp"),
        P("sp", "tp"),
        P(None, "tp"),
        P(None, "tp"),
        P("tp", "sp"),
    )
    return jax.shard_map(
        per_device,
        mesh=mesh,
        in_specs=placed,
        out_specs=P(("grp", "tp"), "sp", None),
        check_vma=False,
    )
```

```python
import math

import jax
import jax.numpy as jnp
from jax import lax
from jax.experimental import pallas as pl
from jax.experimental.pallas import tpu as pltpu
from jax.sharding import PartitionSpec as P

NORM_EPS = 1e-06
ROPE_BASE = 500000.0
LOG2E = math.log2(math.e)
DOC_SPAN = 1024
KEY_UP = 4096.0
VAL_UP = 8192.0
LANES = 128
EDGE = 8
AHEAD = 3


def shifted(array, axis, by):
    length = lax.axis_size(axis)
    return lax.ppermute(array, axis, [(i, (i + by) % length) for i in range(length)])


def from_behind(array, axis):
    length = lax.axis_size(axis)
    return lax.ppermute(array, axis, [(i, i + 1) for i in range(length - 1)])


def turn_tables(positions, width):
    half = width // 2
    freqs = ROPE_BASE ** (-jnp.arange(half, dtype=jnp.float32) * 2.0 / width)
    angles = positions.astype(jnp.float32)[:, None] * freqs[None, :]
    cosine = jnp.cos(angles)
    sine = jnp.sin(angles)
    times = LANES // width
    return (
        jnp.tile(jnp.concatenate([cosine, cosine], axis=1), (1, times)),
        jnp.tile(jnp.concatenate([-sine, sine], axis=1), (1, times)),
    )


def attend(place, q_one, q_two, window, cosine, sine, docs, gain, lam, out_weight, after):
    seqs, rows, q_lanes = q_one.shape
    ranks, per_rank, _ = window.shape
    keys = ranks * rows
    heads = lam.shape[0]
    width = q_lanes // heads
    half = width // 2
    kv_heads = 2
    group = heads // kv_heads
    head_width = LANES // kv_heads
    mult = width ** (-0.5) * LOG2E
    model = out_weight.shape[1]

    def body(
        place_ref, lam_ref, q1_ref, q2_ref, w_ref, c_ref, s_ref, d_ref, g_ref, p_ref, _,
        o_ref, m_ref, h_ref,
    ):
        s = place_ref[0]
        first_key = place_ref[1]
        first_row = place_ref[2]
        lane = lax.broadcasted_iota(jnp.int32, (rows, LANES), 1)
        low = (lane % width) < half
        cos = c_ref[...]
        sin = s_ref[...]
        gain_row = jnp.concatenate([g_ref[...], g_ref[...]], axis=1)
        these = pl.ds(pl.multiple_of(s * rows, rows), rows)
        k_all = w_ref[:, these, 0:LANES].reshape(keys, LANES)
        v_all = w_ref[:, these, LANES : 2 * LANES].reshape(keys, LANES)
        v_ext = jnp.concatenate([v_all, jnp.ones((keys, LANES), jnp.bfloat16)], axis=1)

        placed = []
        for ref in (q1_ref, q2_ref):
            tiles = []
            for h in range(kv_heads):
                x = ref[s, :, h * LANES : (h + 1) * LANES].astype(jnp.float32)
                swap = jnp.where(low, pltpu.roll(x, LANES - half, 1), pltpu.roll(x, half, 1))
                tiles.append((x * cos + swap * sin).astype(jnp.bfloat16).astype(jnp.float32))
            placed.append(tiles)

        def scores(h, c):
            target = c * kv_heads + h
            inside = (lane // width) == target
            parts = []
            for g in range(group):
                by = (width * (target - g)) % LANES
                x = placed[c][h]
                x = pltpu.roll(x, by, 1) if by else x
                parts.append(jnp.where(inside, x, 0.0).astype(jnp.bfloat16))
            q = jnp.concatenate(parts, axis=0)
            return lax.dot_general(
                q, k_all, (((1,), (1,)), ((), ())), preferred_element_type=jnp.float32
            )

        key_pos = first_key + lax.broadcasted_iota(jnp.int32, (rows, keys), 1)
        row_pos = first_row + lax.broadcasted_iota(jnp.int32, (rows, keys), 0)
        even_lane = lax.broadcasted_iota(jnp.int32, (1, LANES), 1) < rows
        this_row = lax.broadcasted_iota(jnp.int32, (EDGE, LANES), 0) == s
        pieces = []
        for i in range(ranks // 2):
            two = [
                jnp.sum(
                    jnp.where(this_row, w_ref[2 * i + b, seqs * rows : per_rank, 0:LANES].astype(jnp.float32), 0.0),
                    axis=0,
                    keepdims=True,
                )
                for b in range(2)
            ]
            pieces.append(jnp.where(even_lane, two[0], two[1]))
        key_doc = jnp.concatenate(pieces, axis=1)
        diagonal = lax.broadcasted_iota(jnp.int32, (rows, rows), 0) == lax.broadcasted_iota(
            jnp.int32, (rows, rows), 1
        )
        row_doc = jnp.sum(
            jnp.where(diagonal, d_ref[pl.ds(s, 1), :].astype(jnp.float32), 0.0),
            axis=1,
            keepdims=True,
        )
        equal = key_doc == row_doc
        bias = jnp.where((key_pos <= row_pos) & equal, 0.0, -1e30)
        ones_back = [
            jnp.sum(
                jnp.where(equal & (key_pos == row_pos - by), 1.0, 0.0), axis=1, keepdims=True
            )
            for by in (1, 2)
        ]
        m_ref[...] = jnp.where(lane == 0, ones_back[0], ones_back[1])

        pairs = [(h, c) for h in range(kv_heads) for c in range(2)]
        upcoming = scores(*pairs[0])
        results = []
        for at in range(len(pairs)):
            score = upcoming
            if at + 1 < len(pairs):
                upcoming = scores(*pairs[at + 1])
            score = score.reshape(group, rows, keys) + bias[None]
            peak = jnp.max(score, axis=-1, keepdims=True)
            expd = jnp.exp2((score - peak) * mult).astype(jnp.bfloat16)
            both = jnp.dot(
                expd.reshape(group * rows, keys), v_ext, preferred_element_type=jnp.float32
            )
            results.append(both[:, :LANES] / both[:, LANES:])
        for h in range(kv_heads):
            here = (lane // head_width) == h
            outs = []
            for g in range(group):
                a = results[2 * h][g * rows : (g + 1) * rows]
                b = results[2 * h + 1][g * rows : (g + 1) * rows]
                o = jnp.where(here, a - lam_ref[h * group + g] * b, 0.0)
                meansq = jnp.sum(o * o, axis=-1, keepdims=True) * (1.0 / head_width)
                o = o * lax.rsqrt(meansq + NORM_EPS) * gain_row
                if (g % 2) != h:
                    o = pltpu.roll(o, head_width, 1)
                outs.append(o)
            for j in range(group // 2):
                tile = (h * group) // 2 + j
                h_ref[:, tile * LANES : (tile + 1) * LANES] = (
                    outs[2 * j] + outs[2 * j + 1]
                ).astype(jnp.bfloat16)
        o_ref[...] = jnp.dot(
            h_ref[...], p_ref[...], preferred_element_type=jnp.float32
        ).astype(jnp.bfloat16)

    smem = pl.BlockSpec(memory_space=pltpu.SMEM)
    vmem = pl.BlockSpec(memory_space=pltpu.VMEM)
    return pl.pallas_call(
        body,
        out_shape=(
            jax.ShapeDtypeStruct((rows, model), jnp.bfloat16),
            jax.ShapeDtypeStruct((rows, LANES), jnp.float32),
        ),
        in_specs=[smem, smem] + [vmem] * 8 + [pl.BlockSpec(memory_space=pl.ANY)],
        out_specs=(vmem, vmem),
        scratch_shapes=[pltpu.VMEM((rows, heads * head_width), jnp.bfloat16)],
        compiler_params=pltpu.CompilerParams(vmem_limit_bytes=24 * 1024 * 1024),
        cost_estimate=pl.CostEstimate(
            flops=3_000_000_000, transcendentals=0, bytes_accessed=4_000_000
        ),
        name="attend",
    )(place, lam, q_one, q_two, window, cosine, sine, docs, gain, out_weight, after)


def feed_forward(blocks, edges, same, weights, conv_gate, conv_value):
    rows, width = blocks[0].shape
    count = len(blocks)
    span = rows + EDGE
    total = span * count
    hidden = conv_gate.shape[1]
    step = 2 * LANES
    cuts = [(a, min(a + step, hidden)) for a in range(0, hidden, step)]
    out_step = 4 * LANES

    def body(*refs):
        x_in, e_in, m_in = refs[:count], refs[count : 2 * count], refs[2 * count : 3 * count]
        cg_ref, cv_ref, w_hbm = refs[3 * count : 3 * count + 3]
        outs = refs[3 * count + 3 : 4 * count + 3]
        x_ref, w_ref, h_ref, b_ref, sems = refs[4 * count + 3 :]

        def piece(at, low, high, base, a, b):
            spot = (slice(low, high), slice(base + a, base + b))
            return pltpu.make_async_copy(w_hbm.at[spot], w_ref.at[spot], sems.at[at])

        queue = []
        for j, (a, b) in enumerate(cuts):
            queue.append([piece(2 * j + n, 0, width, n * hidden, a, b) for n in range(2)])
        for j in range(0, width, out_step):
            queue.append(
                [piece(2 * len(cuts) + j // out_step, j, j + out_step, 2 * hidden, 0, hidden)]
            )

        def launch(at):
            if at < len(queue):
                for copy in queue[at]:
                    copy.start()

        def arrive(at):
            for copy in queue[at]:
                copy.wait()
            launch(at + AHEAD)

        for at in range(AHEAD):
            launch(at)
        for k in range(count):
            x_ref[k * span : k * span + EDGE, :] = e_in[k][...]
            x_ref[k * span + EDGE : (k + 1) * span, :] = x_in[k][...]
            b_ref[k * span : k * span + EDGE, :] = jnp.zeros((EDGE, LANES), jnp.float32)
            b_ref[k * span + EDGE : (k + 1) * span, :] = m_in[k][...]
        one_back = b_ref[:, 0:1]
        two_back = b_ref[:, 1:2]

        def raised(j):
            a, b = cuts[j]
            arrive(j)
            return [
                jnp.dot(
                    x_ref[...], w_ref[:, base + a : base + b], preferred_element_type=jnp.float32
                ).astype(jnp.bfloat16)
                for base in (0, hidden)
            ]

        upcoming = raised(0)
        for j in range(len(cuts)):
            a, b = cuts[j]
            current = upcoming
            if j + 1 < len(cuts):
                upcoming = raised(j + 1)
            convs = []
            for u, taps in zip(current, (cg_ref, cv_ref)):
                u = u.astype(jnp.float32)
                convs.append(
                    taps[2:3, a:b] * u
                    + taps[1:2, a:b] * (one_back * pltpu.roll(u, 1, 0))
                    + taps[0:1, a:b] * (two_back * pltpu.roll(u, 2, 0))
                )
            g, v = convs
            act = g / (1.0 + jnp.exp(-g)) * v
            for k in range(count):
                h_ref[k * rows : (k + 1) * rows, a:b] = act[
                    k * span + EDGE : (k + 1) * span
                ].astype(jnp.bfloat16)
        for a in range(0, width, out_step):
            arrive(len(cuts) + a // out_step)
            part = lax.dot_general(
                h_ref[...],
                w_ref[a : a + out_step, 2 * hidden : 3 * hidden],
                (((1,), (1,)), ((), ())),
                preferred_element_type=jnp.float32,
            ).astype(jnp.bfloat16)
            for k in range(count):
                outs[k][:, a : a + out_step] = part[k * rows : (k + 1) * rows]

    vmem = pl.BlockSpec(memory_space=pltpu.VMEM)
    return pl.pallas_call(
        body,
        out_shape=[jax.ShapeDtypeStruct((rows, width), jnp.bfloat16)] * count,
        in_specs=[vmem] * (3 * count + 2) + [pl.BlockSpec(memory_space=pltpu.HBM)],
        out_specs=[vmem] * count,
        scratch_shapes=[
            pltpu.VMEM((total, width), jnp.bfloat16),
            pltpu.VMEM((width, 3 * hidden), jnp.bfloat16),
            pltpu.VMEM((count * rows, hidden), jnp.bfloat16),
            pltpu.VMEM((total, LANES), jnp.float32),
            pltpu.SemaphoreType.DMA((2 * len(cuts) + width // out_step,)),
        ],
        compiler_params=pltpu.CompilerParams(vmem_limit_bytes=48 * 1024 * 1024),
        name="feed_forward",
    )(*blocks, *edges, *same, conv_gate, conv_value, weights)


def per_device(
    resid_in,
    query_one,
    key_one,
    query_two,
    key_two,
    value,
    lam,
    head_gain,
    doc_ids,
    out_weight,
    norm_gain,
    gate_weight,
    value_weight,
    conv_gate,
    conv_value,
    down_weight,
):
    seqs, rows, q_lanes = query_one.shape
    width = q_lanes // lam.shape[0]
    rank = lax.axis_index("sp")
    ranks = lax.axis_size("sp")
    own = lax.axis_index("tp")
    parts = lax.axis_size("tp")
    model = resid_in.shape[2]

    packed = jnp.concatenate([gate_weight, value_weight, down_weight.T], axis=1)
    weights = lax.all_gather(packed, "sp", axis=0, tiled=True)

    positions = rank * rows + jnp.arange(rows, dtype=jnp.int32)
    cosine, sine = turn_tables(positions, width)
    keys = jnp.concatenate([key_one, key_two], axis=2).astype(jnp.float32)
    half = width // 2
    low = (jnp.arange(LANES) % width) < half
    swap = jnp.where(low, jnp.roll(keys, -half, axis=2), jnp.roll(keys, half, axis=2))
    keys = (keys * cosine + swap * sine).astype(jnp.bfloat16).astype(jnp.float32) * KEY_UP
    vals = value.astype(jnp.float32) * VAL_UP
    body_rows = jnp.concatenate([keys, vals], axis=2).reshape(seqs * rows, 2 * LANES)
    doc_rows = jnp.tile(doc_ids.astype(jnp.float32) * KEY_UP, (1, 2 * LANES // rows))
    doc_rows = jnp.pad(doc_rows, ((0, EDGE - seqs), (0, 0)))
    sent = jnp.concatenate([body_rows, doc_rows], axis=0).astype(jnp.float16)
    everyone = lax.all_gather(sent, "sp", axis=0, tiled=False)

    back = DOC_SPAN // rows
    span = min(back + 2, ranks)
    first = jnp.clip(rank // 2 * 2 - back, 0, ranks - span)
    lanes_down = jnp.where(jnp.arange(2 * LANES) < LANES, 1.0 / KEY_UP, 1.0 / VAL_UP)
    window = lax.dynamic_slice_in_dim(everyone, first, span, 0)
    window = (window.astype(jnp.float32) * lanes_down).astype(jnp.bfloat16)
    gain = head_gain.reshape(1, -1)
    proj = [None] * parts
    same = [None] * parts
    after = lam
    farthest_first = sorted(range(parts), key=lambda k: -min(k, parts - k))
    for k in farthest_first:
        place = jnp.stack([(own + k) % parts, first * rows, rank * rows]).astype(jnp.int32)
        proj[k], same[-k] = attend(
            place, query_one, query_two, window, cosine, sine, doc_ids, gain, lam, out_weight, after
        )
        after = proj[k]
    mid = resid_in[0].astype(jnp.float32) + proj[0].astype(jnp.float32)
    for k in range(1, parts):
        mid = mid + shifted(proj[k], "tp", k).astype(jnp.float32)
    meansq = jnp.mean(mid * mid, axis=-1, keepdims=True)
    normed = (mid * lax.rsqrt(meansq + NORM_EPS) * norm_gain).astype(jnp.bfloat16)
    edge = from_behind(normed[rows - EDGE :], "sp")
    blocks = [normed] + [shifted(normed, "tp", k) for k in range(1, parts)]
    edges = [edge] + [shifted(edge, "tp", k) for k in range(1, parts)]
    partial = feed_forward(blocks, edges, same, weights, conv_gate, conv_value)
    out = mid + partial[0].astype(jnp.float32)
    for k in range(1, parts):
        out = out + shifted(partial[k], "tp", -k).astype(jnp.float32)
    return out.astype(jnp.bfloat16)[None]


def solution(mesh):
    placed = (
        P(("grp", "tp"), "sp", None),
        P("grp", "sp", "tp"),
        P("grp", "sp", "tp"),
        P("grp", "sp", "tp"),
        P("grp", "sp", "tp"),
        P("grp", "sp", "tp"),
        P("tp"),
        P(),
        P("grp", "sp"),
        P("tp", None),
        P(),
        P("sp", "tp"),
        P("sp", "tp"),
        P(None, "tp"),
        P(None, "tp"),
        P("tp", "sp"),
    )
    return jax.shard_map(
        per_device,
        mesh=mesh,
        in_specs=placed,
        out_specs=P(("grp", "tp"), "sp", None),
        check_vma=False,
    )
```

```python
import math

import jax
import jax.numpy as jnp
from jax import lax
from jax.experimental import pallas as pl
from jax.experimental.pallas import tpu as pltpu
from jax.sharding import PartitionSpec as P


NORM_EPS = 1e-06
ROPE_BASE = 500000.0
LOG2E = math.log2(math.e)
DOC_SPAN = 1024
KEY_UP = 4096.0
VAL_UP = 8192.0
LANES = 128
EDGE = 8
WEIGHT_UP = 262144.0
AHEAD = 3


def shifted(array, axis, by):
    length = lax.axis_size(axis)
    return lax.ppermute(array, axis, [(i, (i + by) % length) for i in range(length)])


def from_behind(array, axis):
    length = lax.axis_size(axis)
    return lax.ppermute(array, axis, [(i, i + 1) for i in range(length - 1)])


def turn_tables(positions, width):
    half = width // 2
    freqs = ROPE_BASE ** (-jnp.arange(half, dtype=jnp.float32) * 2.0 / width)
    angles = positions.astype(jnp.float32)[:, None] * freqs[None, :]
    cosine = jnp.cos(angles)
    sine = jnp.sin(angles)
    times = LANES // width
    return (
        jnp.tile(jnp.concatenate([cosine, cosine], axis=1), (1, times)),
        jnp.tile(jnp.concatenate([-sine, sine], axis=1), (1, times)),
    )


def attend(place, q_one, q_two, window, cosine, sine, docs, gain, lam, out_weight, after):
    seqs, rows, q_lanes = q_one.shape
    ranks, per_rank, _ = window.shape
    keys = ranks * rows
    heads = lam.shape[0]
    width = q_lanes // heads
    half = width // 2
    kv_heads = 2
    group = heads // kv_heads
    head_width = LANES // kv_heads
    mult = width ** (-0.5) * LOG2E
    model = out_weight.shape[1]

    def body(
        place_ref, lam_ref, q1_ref, q2_ref, w_ref, c_ref, s_ref, d_ref, g_ref, p_ref, _,
        o_ref, m_ref, h_ref,
    ):
        s = place_ref[0]
        first_key = place_ref[1]
        first_row = place_ref[2]
        lane = lax.broadcasted_iota(jnp.int32, (rows, LANES), 1)
        low = (lane % width) < half
        cos = c_ref[...]
        sin = s_ref[...]
        gain_row = jnp.concatenate([g_ref[...], g_ref[...]], axis=1)
        these = pl.ds(pl.multiple_of(s * rows, rows), rows)
        k_all = w_ref[:, these, 0:LANES].reshape(keys, LANES)
        v_all = w_ref[:, these, LANES : 2 * LANES].reshape(keys, LANES)
        v_ext = jnp.concatenate([v_all, jnp.ones((keys, LANES), jnp.bfloat16)], axis=1)

        placed = []
        for ref in (q1_ref, q2_ref):
            tiles = []
            for h in range(kv_heads):
                x = ref[s, :, h * LANES : (h + 1) * LANES].astype(jnp.float32)
                swap = jnp.where(low, pltpu.roll(x, LANES - half, 1), pltpu.roll(x, half, 1))
                tiles.append((x * cos + swap * sin).astype(jnp.bfloat16).astype(jnp.float32))
            placed.append(tiles)

        def scores(h, c):
            target = c * kv_heads + h
            inside = (lane // width) == target
            parts = []
            for g in range(group):
                by = (width * (target - g)) % LANES
                x = placed[c][h]
                x = pltpu.roll(x, by, 1) if by else x
                parts.append(jnp.where(inside, x, 0.0).astype(jnp.bfloat16))
            q = jnp.concatenate(parts, axis=0)
            return lax.dot_general(
                q, k_all, (((1,), (1,)), ((), ())), preferred_element_type=jnp.float32
            )

        key_pos = first_key + lax.broadcasted_iota(jnp.int32, (rows, keys), 1)
        row_pos = first_row + lax.broadcasted_iota(jnp.int32, (rows, keys), 0)
        even_lane = lax.broadcasted_iota(jnp.int32, (1, LANES), 1) < rows
        this_row = lax.broadcasted_iota(jnp.int32, (EDGE, LANES), 0) == s
        pieces = []
        for i in range(ranks // 2):
            two = [
                jnp.sum(
                    jnp.where(this_row, w_ref[2 * i + b, seqs * rows : per_rank, 0:LANES].astype(jnp.float32), 0.0),
                    axis=0,
                    keepdims=True,
                )
                for b in range(2)
            ]
            pieces.append(jnp.where(even_lane, two[0], two[1]))
        key_doc = jnp.concatenate(pieces, axis=1)
        diagonal = lax.broadcasted_iota(jnp.int32, (rows, rows), 0) == lax.broadcasted_iota(
            jnp.int32, (rows, rows), 1
        )
        row_doc = jnp.sum(
            jnp.where(diagonal, d_ref[pl.ds(s, 1), :].astype(jnp.float32), 0.0),
            axis=1,
            keepdims=True,
        )
        equal = key_doc == row_doc
        bias = jnp.where((key_pos <= row_pos) & equal, 0.0, -1e30)
        ones_back = [
            jnp.sum(
                jnp.where(equal & (key_pos == row_pos - by), 1.0, 0.0), axis=1, keepdims=True
            )
            for by in (1, 2)
        ]
        m_ref[...] = jnp.where(lane == 0, ones_back[0], ones_back[1])

        pairs = [(h, c) for h in range(kv_heads) for c in range(2)]
        upcoming = scores(*pairs[0])
        results = []
        for at in range(len(pairs)):
            score = upcoming
            if at + 1 < len(pairs):
                upcoming = scores(*pairs[at + 1])
            score = score.reshape(group, rows, keys) + bias[None]
            peak = jnp.max(score, axis=-1, keepdims=True)
            expd = jnp.exp2((score - peak) * mult).astype(jnp.bfloat16)
            both = jnp.dot(
                expd.reshape(group * rows, keys), v_ext, preferred_element_type=jnp.float32
            )
            results.append(both[:, :LANES] / both[:, LANES:])
        for h in range(kv_heads):
            here = (lane // head_width) == h
            outs = []
            for g in range(group):
                a = results[2 * h][g * rows : (g + 1) * rows]
                b = results[2 * h + 1][g * rows : (g + 1) * rows]
                o = jnp.where(here, a - lam_ref[h * group + g] * b, 0.0)
                meansq = jnp.sum(o * o, axis=-1, keepdims=True) * (1.0 / head_width)
                o = o * lax.rsqrt(meansq + NORM_EPS) * gain_row
                if (g % 2) != h:
                    o = pltpu.roll(o, head_width, 1)
                outs.append(o)
            for j in range(group // 2):
                tile = (h * group) // 2 + j
                h_ref[:, tile * LANES : (tile + 1) * LANES] = (
                    outs[2 * j] + outs[2 * j + 1]
                ).astype(jnp.bfloat16)
        o_ref[...] = jnp.dot(
            h_ref[...], p_ref[...], preferred_element_type=jnp.float32
        ).astype(jnp.bfloat16)

    smem = pl.BlockSpec(memory_space=pltpu.SMEM)
    vmem = pl.BlockSpec(memory_space=pltpu.VMEM)
    return pl.pallas_call(
        body,
        out_shape=(
            jax.ShapeDtypeStruct((rows, model), jnp.bfloat16),
            jax.ShapeDtypeStruct((rows, LANES), jnp.float32),
        ),
        in_specs=[smem, smem] + [vmem] * 8 + [pl.BlockSpec(memory_space=pl.ANY)],
        out_specs=(vmem, vmem),
        scratch_shapes=[pltpu.VMEM((rows, heads * head_width), jnp.bfloat16)],
        compiler_params=pltpu.CompilerParams(vmem_limit_bytes=24 * 1024 * 1024),
        cost_estimate=pl.CostEstimate(
            flops=3_000_000_000, transcendentals=0, bytes_accessed=4_000_000
        ),
        name="attend",
    )(place, lam, q_one, q_two, window, cosine, sine, docs, gain, out_weight, after)


def feed_forward(blocks, edges, same, early, weights, conv_gate, conv_value):
    rows, width = blocks[0].shape
    count = len(blocks)
    span = rows + EDGE
    total = span * count
    hidden = conv_gate.shape[1]
    step = 2 * LANES
    ready = early.shape[1] // 2
    later = hidden - ready
    bounds = [0, ready] + list(range(ready + step, hidden + 1, step))
    assert bounds[-1] == hidden and ready % LANES == 0
    cuts = list(zip(bounds[:-1], bounds[1:]))
    out_step = 16 * LANES

    def body(*refs):
        x_in, e_in, m_in = refs[:count], refs[count : 2 * count], refs[2 * count : 3 * count]
        cg_ref, cv_ref, early_ref, w_hbm = refs[3 * count : 3 * count + 4]
        outs = refs[3 * count + 4 : 4 * count + 4]
        x_ref, w_ref, h_ref, b_ref, sems = refs[4 * count + 4 :]

        def piece(at, low, high, base, a, b):
            spot = (slice(low, high), slice(base + a, base + b))
            return pltpu.make_async_copy(w_hbm.at[spot], w_ref.at[spot], sems.at[at])

        queue = []
        for j, (a, b) in enumerate(cuts[1:]):
            a, b = a - ready, b - ready
            queue.append([piece(2 * j + n, 0, width, n * later, a, b) for n in range(2)])
        for j in range(0, width, out_step):
            queue.append(
                [piece(2 * len(cuts) + j // out_step, j, j + out_step, 2 * later, 0, hidden)]
            )

        def launch(at):
            if at < len(queue):
                for copy in queue[at]:
                    copy.start()

        def arrive(at):
            for copy in queue[at]:
                copy.wait()
            launch(at + AHEAD)

        for at in range(AHEAD):
            launch(at)
        for k in range(count):
            x_ref[k * span : k * span + EDGE, :] = e_in[k][...]
            x_ref[k * span + EDGE : (k + 1) * span, :] = x_in[k][...]
            b_ref[k * span : k * span + EDGE, :] = jnp.zeros((EDGE, LANES), jnp.float32)
            b_ref[k * span + EDGE : (k + 1) * span, :] = m_in[k][...]
        one_back = b_ref[:, 0:1]
        two_back = b_ref[:, 1:2]

        def raised(j):
            a, b = cuts[j]
            if j:
                arrive(j - 1)
                a, b = a - ready, b - ready
            source, far = (w_ref, later) if j else (early_ref, ready)
            return [
                jnp.dot(
                    x_ref[...], source[:, base + a : base + b], preferred_element_type=jnp.float32
                ).astype(jnp.bfloat16)
                for base in (0, far)
            ]

        upcoming = raised(0)
        for j in range(len(cuts)):
            a, b = cuts[j]
            current = upcoming
            if j + 1 < len(cuts):
                upcoming = raised(j + 1)
            convs = []
            for u, taps in zip(current, (cg_ref, cv_ref)):
                u = u.astype(jnp.float32)
                convs.append(
                    taps[2:3, a:b] * u
                    + taps[1:2, a:b] * (one_back * pltpu.roll(u, 1, 0))
                    + taps[0:1, a:b] * (two_back * pltpu.roll(u, 2, 0))
                )
            g, v = convs
            act = g / (1.0 + jnp.exp(-g)) * v
            for k in range(count):
                h_ref[k * rows : (k + 1) * rows, a:b] = act[
                    k * span + EDGE : (k + 1) * span
                ].astype(jnp.bfloat16)
        for a in range(0, width, out_step):
            arrive(len(cuts) - 1 + a // out_step)
            part = lax.dot_general(
                h_ref[...],
                w_ref[a : a + out_step, 2 * later : 2 * later + hidden],
                (((1,), (1,)), ((), ())),
                preferred_element_type=jnp.float32,
            ).astype(jnp.bfloat16)
            for k in range(count):
                outs[k][:, a : a + out_step] = part[k * rows : (k + 1) * rows]

    vmem = pl.BlockSpec(memory_space=pltpu.VMEM)
    return pl.pallas_call(
        body,
        out_shape=[jax.ShapeDtypeStruct((rows, width), jnp.bfloat16)] * count,
        in_specs=[vmem] * (3 * count + 3) + [pl.BlockSpec(memory_space=pltpu.HBM)],
        out_specs=[vmem] * count,
        scratch_shapes=[
            pltpu.VMEM((total, width), jnp.bfloat16),
            pltpu.VMEM((width, 2 * later + hidden), jnp.bfloat16),
            pltpu.VMEM((count * rows, hidden), jnp.bfloat16),
            pltpu.VMEM((total, LANES), jnp.float32),
            pltpu.SemaphoreType.DMA((2 * len(cuts) + width // out_step,)),
        ],
        compiler_params=pltpu.CompilerParams(vmem_limit_bytes=48 * 1024 * 1024),
        name="feed_forward",
    )(*blocks, *edges, *same, conv_gate, conv_value, early, weights)


def per_device(
    resid_in,
    query_one,
    key_one,
    query_two,
    key_two,
    value,
    lam,
    head_gain,
    doc_ids,
    out_weight,
    norm_gain,
    gate_weight,
    value_weight,
    conv_gate,
    conv_value,
    down_weight,
):
    seqs, rows, q_lanes = query_one.shape
    width = q_lanes // lam.shape[0]
    rank = lax.axis_index("sp")
    ranks = lax.axis_size("sp")
    own = lax.axis_index("tp")
    parts = lax.axis_size("tp")
    model = resid_in.shape[2]

    packed = jnp.concatenate(
        [gate_weight[:, LANES:], value_weight[:, LANES:], down_weight.T], axis=1
    )
    weights = lax.all_gather(packed, "sp", axis=0, tiled=True)

    positions = rank * rows + jnp.arange(rows, dtype=jnp.int32)
    cosine, sine = turn_tables(positions, width)
    keys = jnp.concatenate([key_one, key_two], axis=2).astype(jnp.float32)
    half = width // 2
    low = (jnp.arange(LANES) % width) < half
    swap = jnp.where(low, jnp.roll(keys, -half, axis=2), jnp.roll(keys, half, axis=2))
    keys = (keys * cosine + swap * sine).astype(jnp.bfloat16).astype(jnp.float32) * KEY_UP
    vals = value.astype(jnp.float32) * VAL_UP
    body_rows = jnp.concatenate([keys, vals], axis=2).reshape(seqs * rows, 2 * LANES)
    doc_rows = jnp.tile(doc_ids.astype(jnp.float32) * KEY_UP, (1, 2 * LANES // rows))
    doc_rows = jnp.pad(doc_rows, ((0, EDGE - seqs), (0, 0)))
    first_weights = jnp.concatenate([gate_weight[:, :LANES], value_weight[:, :LANES]], axis=1)
    first_weights = first_weights.astype(jnp.float32) * WEIGHT_UP
    sent = jnp.concatenate([body_rows, doc_rows, first_weights], axis=0).astype(jnp.float16)
    everyone = lax.all_gather(sent, "sp", axis=0, tiled=False)

    back = DOC_SPAN // rows
    span = min(back + 2, ranks)
    first = jnp.clip(rank // 2 * 2 - back, 0, ranks - span)
    lanes_down = jnp.where(jnp.arange(2 * LANES) < LANES, 1.0 / KEY_UP, 1.0 / VAL_UP)
    known = seqs * rows + EDGE
    early = everyone[:, known:].reshape(model, 2 * LANES)
    early = (early.astype(jnp.float32) * (1.0 / WEIGHT_UP)).astype(jnp.bfloat16)
    window = lax.dynamic_slice(everyone, (first, 0, 0), (span, known, 2 * LANES))
    window = (window.astype(jnp.float32) * lanes_down).astype(jnp.bfloat16)
    gain = head_gain.reshape(1, -1)
    proj = [None] * parts
    same = [None] * parts
    after = lam
    farthest_first = sorted(range(parts), key=lambda k: -min(k, parts - k))
    for k in farthest_first:
        place = jnp.stack([(own + k) % parts, first * rows, rank * rows]).astype(jnp.int32)
        proj[k], same[-k] = attend(
            place, query_one, query_two, window, cosine, sine, doc_ids, gain, lam, out_weight, after
        )
        after = proj[k]
    mid = resid_in[0].astype(jnp.float32) + proj[0].astype(jnp.float32)
    for k in range(1, parts):
        mid = mid + shifted(proj[k], "tp", k).astype(jnp.float32)
    meansq = jnp.mean(mid * mid, axis=-1, keepdims=True)
    normed = (mid * lax.rsqrt(meansq + NORM_EPS) * norm_gain).astype(jnp.bfloat16)
    edge = from_behind(normed[rows - EDGE :], "sp")
    blocks = [normed] + [shifted(normed, "tp", k) for k in range(1, parts)]
    edges = [edge] + [shifted(edge, "tp", k) for k in range(1, parts)]
    partial = feed_forward(blocks, edges, same, early, weights, conv_gate, conv_value)
    out = mid + partial[0].astype(jnp.float32)
    for k in range(1, parts):
        out = out + shifted(partial[k], "tp", -k).astype(jnp.float32)
    return out.astype(jnp.bfloat16)[None]


def solution(mesh):
    placed = (
        P(("grp", "tp"), "sp", None),
        P("grp", "sp", "tp"),
        P("grp", "sp", "tp"),
        P("grp", "sp", "tp"),
        P("grp", "sp", "tp"),
        P("grp", "sp", "tp"),
        P("tp"),
        P(),
        P("grp", "sp"),
        P("tp", None),
        P(),
        P("sp", "tp"),
        P("sp", "tp"),
        P(None, "tp"),
        P(None, "tp"),
        P("tp", "sp"),
    )

    return jax.shard_map(
        per_device,
        mesh=mesh,
        in_specs=placed,
        out_specs=P(("grp", "tp"), "sp", None),
        check_vma=False,
    )
```

```python
import math

import jax
import jax.numpy as jnp
from jax import lax
from jax.experimental import pallas as pl
from jax.experimental.pallas import tpu as pltpu
from jax.sharding import PartitionSpec as P

NORM_EPS = 1e-06
ROPE_BASE = 500000.0
LOG2E = math.log2(math.e)
DOC_SPAN = 1024
KEY_UP = 4096.0
VAL_UP = 8192.0
LANES = 128
EDGE = 8
AHEAD = 3


def shifted(array, axis, by):
    length = lax.axis_size(axis)
    return lax.ppermute(array, axis, [(i, (i + by) % length) for i in range(length)])


def from_behind(array, axis):
    length = lax.axis_size(axis)
    return lax.ppermute(array, axis, [(i, i + 1) for i in range(length - 1)])


def turn_tables(positions, width):
    half = width // 2
    freqs = ROPE_BASE ** (-jnp.arange(half, dtype=jnp.float32) * 2.0 / width)
    angles = positions.astype(jnp.float32)[:, None] * freqs[None, :]
    cosine = jnp.cos(angles)
    sine = jnp.sin(angles)
    times = LANES // width
    return (
        jnp.tile(jnp.concatenate([cosine, cosine], axis=1), (1, times)),
        jnp.tile(jnp.concatenate([-sine, sine], axis=1), (1, times)),
    )


def attend(place, q_one, q_two, window, cosine, sine, docs, gain, lam, out_weight, after):
    seqs, rows, q_lanes = q_one.shape
    ranks, per_rank, _ = window.shape
    keys = ranks * rows
    heads = lam.shape[0]
    width = q_lanes // heads
    half = width // 2
    kv_heads = 2
    group = heads // kv_heads
    head_width = LANES // kv_heads
    mult = width ** (-0.5) * LOG2E
    model = out_weight.shape[1]

    def body(
        place_ref, lam_ref, q1_ref, q2_ref, w_ref, c_ref, s_ref, d_ref, g_ref, p_ref, _,
        o_ref, m_ref, h_ref,
    ):
        s = place_ref[0]
        first_key = place_ref[1]
        first_row = place_ref[2]
        lane = lax.broadcasted_iota(jnp.int32, (rows, LANES), 1)
        low = (lane % width) < half
        cos = c_ref[...]
        sin = s_ref[...]
        gain_row = jnp.concatenate([g_ref[...], g_ref[...]], axis=1)
        these = pl.ds(pl.multiple_of(s * rows, rows), rows)
        k_all = w_ref[:, these, 0:LANES].reshape(keys, LANES)
        v_all = w_ref[:, these, LANES : 2 * LANES].reshape(keys, LANES)
        v_ext = jnp.concatenate([v_all, jnp.ones((keys, LANES), jnp.bfloat16)], axis=1)

        placed = []
        for ref in (q1_ref, q2_ref):
            tiles = []
            for h in range(kv_heads):
                x = ref[s, :, h * LANES : (h + 1) * LANES].astype(jnp.float32)
                swap = jnp.where(low, pltpu.roll(x, LANES - half, 1), pltpu.roll(x, half, 1))
                tiles.append((x * cos + swap * sin).astype(jnp.bfloat16).astype(jnp.float32))
            placed.append(tiles)

        def scores(h, c):
            target = c * kv_heads + h
            inside = (lane // width) == target
            parts = []
            for g in range(group):
                by = (width * (target - g)) % LANES
                x = placed[c][h]
                x = pltpu.roll(x, by, 1) if by else x
                parts.append(jnp.where(inside, x, 0.0).astype(jnp.bfloat16))
            q = jnp.concatenate(parts, axis=0)
            return lax.dot_general(
                q, k_all, (((1,), (1,)), ((), ())), preferred_element_type=jnp.float32
            )

        key_pos = first_key + lax.broadcasted_iota(jnp.int32, (rows, keys), 1)
        row_pos = first_row + lax.broadcasted_iota(jnp.int32, (rows, keys), 0)
        even_lane = lax.broadcasted_iota(jnp.int32, (1, LANES), 1) < rows
        this_row = lax.broadcasted_iota(jnp.int32, (EDGE, LANES), 0) == s
        pieces = []
        for i in range(ranks // 2):
            two = [
                jnp.sum(
                    jnp.where(this_row, w_ref[2 * i + b, seqs * rows : per_rank, 0:LANES].astype(jnp.float32), 0.0),
                    axis=0,
                    keepdims=True,
                )
                for b in range(2)
            ]
            pieces.append(jnp.where(even_lane, two[0], two[1]))
        key_doc = jnp.concatenate(pieces, axis=1)
        diagonal = lax.broadcasted_iota(jnp.int32, (rows, rows), 0) == lax.broadcasted_iota(
            jnp.int32, (rows, rows), 1
        )
        row_doc = jnp.sum(
            jnp.where(diagonal, d_ref[pl.ds(s, 1), :].astype(jnp.float32), 0.0),
            axis=1,
            keepdims=True,
        )
        equal = key_doc == row_doc
        bias = jnp.where((key_pos <= row_pos) & equal, 0.0, -1e30)
        ones_back = [
            jnp.sum(
                jnp.where(equal & (key_pos == row_pos - by), 1.0, 0.0), axis=1, keepdims=True
            )
            for by in (1, 2)
        ]
        m_ref[...] = jnp.where(lane == 0, ones_back[0], ones_back[1])

        pairs = [(h, c) for h in range(kv_heads) for c in range(2)]
        upcoming = scores(*pairs[0])
        results = []
        for at in range(len(pairs)):
            score = upcoming
            if at + 1 < len(pairs):
                upcoming = scores(*pairs[at + 1])
            score = score.reshape(group, rows, keys) + bias[None]
            peak = jnp.max(score, axis=-1, keepdims=True)
            expd = jnp.exp2((score - peak) * mult).astype(jnp.bfloat16)
            both = jnp.dot(
                expd.reshape(group * rows, keys), v_ext, preferred_element_type=jnp.float32
            )
            results.append(both[:, :LANES] / both[:, LANES:])
        for h in range(kv_heads):
            here = (lane // head_width) == h
            outs = []
            for g in range(group):
                a = results[2 * h][g * rows : (g + 1) * rows]
                b = results[2 * h + 1][g * rows : (g + 1) * rows]
                o = jnp.where(here, a - lam_ref[h * group + g] * b, 0.0)
                meansq = jnp.sum(o * o, axis=-1, keepdims=True) * (1.0 / head_width)
                o = o * lax.rsqrt(meansq + NORM_EPS) * gain_row
                if (g % 2) != h:
                    o = pltpu.roll(o, head_width, 1)
                outs.append(o)
            for j in range(group // 2):
                tile = (h * group) // 2 + j
                h_ref[:, tile * LANES : (tile + 1) * LANES] = (
                    outs[2 * j] + outs[2 * j + 1]
                ).astype(jnp.bfloat16)
        o_ref[...] = jnp.dot(
            h_ref[...], p_ref[...], preferred_element_type=jnp.float32
        ).astype(jnp.bfloat16)

    smem = pl.BlockSpec(memory_space=pltpu.SMEM)
    vmem = pl.BlockSpec(memory_space=pltpu.VMEM)
    return pl.pallas_call(
        body,
        out_shape=(
            jax.ShapeDtypeStruct((rows, model), jnp.bfloat16),
            jax.ShapeDtypeStruct((rows, LANES), jnp.float32),
        ),
        in_specs=[smem, smem] + [vmem] * 8 + [pl.BlockSpec(memory_space=pl.ANY)],
        out_specs=(vmem, vmem),
        scratch_shapes=[pltpu.VMEM((rows, heads * head_width), jnp.bfloat16)],
        compiler_params=pltpu.CompilerParams(vmem_limit_bytes=24 * 1024 * 1024),
        cost_estimate=pl.CostEstimate(
            flops=3_000_000_000, transcendentals=0, bytes_accessed=4_000_000
        ),
        name="attend",
    )(place, lam, q_one, q_two, window, cosine, sine, docs, gain, out_weight, after)


def feed_forward(blocks, edges, same, weights, conv_gate, conv_value):
    rows, width = blocks[0].shape
    count = len(blocks)
    span = rows + EDGE
    total = span * count
    hidden = conv_gate.shape[1]
    step = 2 * LANES
    bounds = [0] + list(range(hidden % step, hidden + 1, step))
    cuts = list(zip(bounds[:-1], bounds[1:]))
    out_step = 16 * LANES

    def body(*refs):
        x_in, e_in, m_in = refs[:count], refs[count : 2 * count], refs[2 * count : 3 * count]
        cg_ref, cv_ref, w_hbm = refs[3 * count : 3 * count + 3]
        outs = refs[3 * count + 3 : 4 * count + 3]
        x_ref, w_ref, h_ref, b_ref, sems = refs[4 * count + 3 :]

        def piece(at, low, high, base, a, b):
            spot = (slice(low, high), slice(base + a, base + b))
            return pltpu.make_async_copy(w_hbm.at[spot], w_ref.at[spot], sems.at[at])

        queue = []
        for j, (a, b) in enumerate(cuts):
            queue.append([piece(2 * j + n, 0, width, n * hidden, a, b) for n in range(2)])
        for j in range(0, width, out_step):
            queue.append(
                [piece(2 * len(cuts) + j // out_step, j, j + out_step, 2 * hidden, 0, hidden)]
            )

        def launch(at):
            if at < len(queue):
                for copy in queue[at]:
                    copy.start()

        def arrive(at):
            for copy in queue[at]:
                copy.wait()
            launch(at + AHEAD)

        for at in range(AHEAD):
            launch(at)
        for k in range(count):
            x_ref[k * span : k * span + EDGE, :] = e_in[k][...]
            x_ref[k * span + EDGE : (k + 1) * span, :] = x_in[k][...]
            b_ref[k * span : k * span + EDGE, :] = jnp.zeros((EDGE, LANES), jnp.float32)
            b_ref[k * span + EDGE : (k + 1) * span, :] = m_in[k][...]
        one_back = b_ref[:, 0:1]
        two_back = b_ref[:, 1:2]

        def raised(j):
            a, b = cuts[j]
            arrive(j)
            return [
                jnp.dot(
                    x_ref[...], w_ref[:, base + a : base + b], preferred_element_type=jnp.float32
                ).astype(jnp.bfloat16)
                for base in (0, hidden)
            ]

        upcoming = raised(0)
        for j in range(len(cuts)):
            a, b = cuts[j]
            current = upcoming
            if j + 1 < len(cuts):
                upcoming = raised(j + 1)
            convs = []
            for u, taps in zip(current, (cg_ref, cv_ref)):
                u = u.astype(jnp.float32)
                convs.append(
                    taps[2:3, a:b] * u
                    + taps[1:2, a:b] * (one_back * pltpu.roll(u, 1, 0))
                    + taps[0:1, a:b] * (two_back * pltpu.roll(u, 2, 0))
                )
            g, v = convs
            act = g / (1.0 + jnp.exp(-g)) * v
            for k in range(count):
                h_ref[k * rows : (k + 1) * rows, a:b] = act[
                    k * span + EDGE : (k + 1) * span
                ].astype(jnp.bfloat16)
        for a in range(0, width, out_step):
            arrive(len(cuts) + a // out_step)
            part = lax.dot_general(
                h_ref[...],
                w_ref[a : a + out_step, 2 * hidden : 3 * hidden],
                (((1,), (1,)), ((), ())),
                preferred_element_type=jnp.float32,
            ).astype(jnp.bfloat16)
            for k in range(count):
                outs[k][:, a : a + out_step] = part[k * rows : (k + 1) * rows]

    vmem = pl.BlockSpec(memory_space=pltpu.VMEM)
    return pl.pallas_call(
        body,
        out_shape=[jax.ShapeDtypeStruct((rows, width), jnp.bfloat16)] * count,
        in_specs=[vmem] * (3 * count + 2) + [pl.BlockSpec(memory_space=pltpu.HBM)],
        out_specs=[vmem] * count,
        scratch_shapes=[
            pltpu.VMEM((total, width), jnp.bfloat16),
            pltpu.VMEM((width, 3 * hidden), jnp.bfloat16),
            pltpu.VMEM((count * rows, hidden), jnp.bfloat16),
            pltpu.VMEM((total, LANES), jnp.float32),
            pltpu.SemaphoreType.DMA((2 * len(cuts) + width // out_step,)),
        ],
        compiler_params=pltpu.CompilerParams(vmem_limit_bytes=48 * 1024 * 1024),
        name="feed_forward",
    )(*blocks, *edges, *same, conv_gate, conv_value, weights)


def per_device(
    resid_in,
    query_one,
    key_one,
    query_two,
    key_two,
    value,
    lam,
    head_gain,
    doc_ids,
    out_weight,
    norm_gain,
    gate_weight,
    value_weight,
    conv_gate,
    conv_value,
    down_weight,
):
    seqs, rows, q_lanes = query_one.shape
    width = q_lanes // lam.shape[0]
    rank = lax.axis_index("sp")
    ranks = lax.axis_size("sp")
    own = lax.axis_index("tp")
    parts = lax.axis_size("tp")
    model = resid_in.shape[2]

    packed = jnp.concatenate([gate_weight, value_weight, down_weight.T], axis=1)
    weights = lax.all_gather(packed, "sp", axis=0, tiled=True)

    positions = rank * rows + jnp.arange(rows, dtype=jnp.int32)
    cosine, sine = turn_tables(positions, width)
    keys = jnp.concatenate([key_one, key_two], axis=2).astype(jnp.float32)
    half = width // 2
    low = (jnp.arange(LANES) % width) < half
    swap = jnp.where(low, jnp.roll(keys, -half, axis=2), jnp.roll(keys, half, axis=2))
    keys = (keys * cosine + swap * sine).astype(jnp.bfloat16).astype(jnp.float32) * KEY_UP
    vals = value.astype(jnp.float32) * VAL_UP
    body_rows = jnp.concatenate([keys, vals], axis=2).reshape(seqs * rows, 2 * LANES)
    doc_rows = jnp.tile(doc_ids.astype(jnp.float32) * KEY_UP, (1, 2 * LANES // rows))
    doc_rows = jnp.pad(doc_rows, ((0, EDGE - seqs), (0, 0)))
    sent = jnp.concatenate([body_rows, doc_rows], axis=0).astype(jnp.float16)
    everyone = lax.all_gather(sent, "sp", axis=0, tiled=False)

    back = DOC_SPAN // rows
    span = min(back + 2, ranks)
    first = jnp.clip(rank // 2 * 2 - back, 0, ranks - span)
    lanes_down = jnp.where(jnp.arange(2 * LANES) < LANES, 1.0 / KEY_UP, 1.0 / VAL_UP)
    window = lax.dynamic_slice_in_dim(everyone, first, span, 0)
    window = (window.astype(jnp.float32) * lanes_down).astype(jnp.bfloat16)
    gain = head_gain.reshape(1, -1)
    proj = [None] * parts
    same = [None] * parts
    after = lam
    farthest_first = sorted(range(parts), key=lambda k: -min(k, parts - k))
    for k in farthest_first:
        place = jnp.stack([(own + k) % parts, first * rows, rank * rows]).astype(jnp.int32)
        proj[k], same[-k] = attend(
            place, query_one, query_two, window, cosine, sine, doc_ids, gain, lam, out_weight, after
        )
        after = proj[k]
    mid = resid_in[0].astype(jnp.float32) + proj[0].astype(jnp.float32)
    for k in range(1, parts):
        mid = mid + shifted(proj[k], "tp", k).astype(jnp.float32)
    meansq = jnp.mean(mid * mid, axis=-1, keepdims=True)
    normed = (mid * lax.rsqrt(meansq + NORM_EPS) * norm_gain).astype(jnp.bfloat16)
    edge = from_behind(normed[rows - EDGE :], "sp")
    blocks = [normed] + [shifted(normed, "tp", k) for k in range(1, parts)]
    edges = [edge] + [shifted(edge, "tp", k) for k in range(1, parts)]
    partial = feed_forward(blocks, edges, same, weights, conv_gate, conv_value)
    out = mid + partial[0].astype(jnp.float32)
    for k in range(1, parts):
        out = out + shifted(partial[k], "tp", -k).astype(jnp.float32)
    return out.astype(jnp.bfloat16)[None]


def solution(mesh):
    placed = (
        P(("grp", "tp"), "sp", None),
        P("grp", "sp", "tp"),
        P("grp", "sp", "tp"),
        P("grp", "sp", "tp"),
        P("grp", "sp", "tp"),
        P("grp", "sp", "tp"),
        P("tp"),
        P(),
        P("grp", "sp"),
        P("tp", None),
        P(),
        P("sp", "tp"),
        P("sp", "tp"),
        P(None, "tp"),
        P(None, "tp"),
        P("tp", "sp"),
    )
    return jax.shard_map(
        per_device,
        mesh=mesh,
        in_specs=placed,
        out_specs=P(("grp", "tp"), "sp", None),
        check_vma=False,
    )
```

```python
import math

import jax
import jax.numpy as jnp
from jax import lax
from jax.experimental import pallas as pl
from jax.experimental.pallas import tpu as pltpu
from jax.sharding import PartitionSpec as P

NORM_EPS = 1e-06
ROPE_BASE = 500000.0
LOG2E = math.log2(math.e)
DOC_SPAN = 1024
KEY_UP = 4096.0
VAL_UP = 8192.0
LANES = 128
EDGE = 8
AHEAD = 3


def shifted(array, axis, by):
    length = lax.axis_size(axis)
    return lax.ppermute(array, axis, [(i, (i + by) % length) for i in range(length)])


def from_behind(array, axis):
    length = lax.axis_size(axis)
    return lax.ppermute(array, axis, [(i, i + 1) for i in range(length - 1)])


def turn_tables(positions, width):
    half = width // 2
    freqs = ROPE_BASE ** (-jnp.arange(half, dtype=jnp.float32) * 2.0 / width)
    angles = positions.astype(jnp.float32)[:, None] * freqs[None, :]
    cosine = jnp.cos(angles)
    sine = jnp.sin(angles)
    times = LANES // width
    return (
        jnp.tile(jnp.concatenate([cosine, cosine], axis=1), (1, times)),
        jnp.tile(jnp.concatenate([-sine, sine], axis=1), (1, times)),
    )


def attend(place, q_one, q_two, window, cosine, sine, docs, gain, lam, out_weight, after):
    seqs, rows, q_lanes = q_one.shape
    ranks, per_rank, _ = window.shape
    keys = ranks * rows
    heads = lam.shape[0]
    width = q_lanes // heads
    half = width // 2
    kv_heads = 2
    group = heads // kv_heads
    head_width = LANES // kv_heads
    mult = width ** (-0.5) * LOG2E
    model = out_weight.shape[1]

    def body(
        place_ref, lam_ref, q1_ref, q2_ref, w_ref, c_ref, s_ref, d_ref, g_ref, p_ref, _,
        o_ref, m_ref, h_ref,
    ):
        s = place_ref[0]
        first_key = place_ref[1]
        first_row = place_ref[2]
        lane = lax.broadcasted_iota(jnp.int32, (rows, LANES), 1)
        low = (lane % width) < half
        cos = c_ref[...]
        sin = s_ref[...]
        gain_row = jnp.concatenate([g_ref[...], g_ref[...]], axis=1)
        these = pl.ds(pl.multiple_of(s * rows, rows), rows)
        k_all = w_ref[:, these, 0:LANES].reshape(keys, LANES)
        v_all = w_ref[:, these, LANES : 2 * LANES].reshape(keys, LANES)
        v_ext = jnp.concatenate([v_all, jnp.ones((keys, LANES), jnp.bfloat16)], axis=1)

        placed = []
        for ref in (q1_ref, q2_ref):
            tiles = []
            for h in range(kv_heads):
                x = ref[s, :, h * LANES : (h + 1) * LANES].astype(jnp.float32)
                swap = jnp.where(low, pltpu.roll(x, LANES - half, 1), pltpu.roll(x, half, 1))
                tiles.append((x * cos + swap * sin).astype(jnp.bfloat16).astype(jnp.float32))
            placed.append(tiles)

        def scores(h, c):
            target = c * kv_heads + h
            inside = (lane // width) == target
            parts = []
            for g in range(group):
                by = (width * (target - g)) % LANES
                x = placed[c][h]
                x = pltpu.roll(x, by, 1) if by else x
                parts.append(jnp.where(inside, x, 0.0).astype(jnp.bfloat16))
            q = jnp.concatenate(parts, axis=0)
            return lax.dot_general(
                q, k_all, (((1,), (1,)), ((), ())), preferred_element_type=jnp.float32
            )

        key_pos = first_key + lax.broadcasted_iota(jnp.int32, (rows, keys), 1)
        row_pos = first_row + lax.broadcasted_iota(jnp.int32, (rows, keys), 0)
        even_lane = lax.broadcasted_iota(jnp.int32, (1, LANES), 1) < rows
        this_row = lax.broadcasted_iota(jnp.int32, (EDGE, LANES), 0) == s
        pieces = []
        for i in range(ranks // 2):
            two = [
                jnp.sum(
                    jnp.where(this_row, w_ref[2 * i + b, seqs * rows : per_rank, 0:LANES].astype(jnp.float32), 0.0),
                    axis=0,
                    keepdims=True,
                )
                for b in range(2)
            ]
            pieces.append(jnp.where(even_lane, two[0], two[1]))
        key_doc = jnp.concatenate(pieces, axis=1)
        diagonal = lax.broadcasted_iota(jnp.int32, (rows, rows), 0) == lax.broadcasted_iota(
            jnp.int32, (rows, rows), 1
        )
        row_doc = jnp.sum(
            jnp.where(diagonal, d_ref[pl.ds(s, 1), :].astype(jnp.float32), 0.0),
            axis=1,
            keepdims=True,
        )
        equal = key_doc == row_doc
        bias = jnp.where((key_pos <= row_pos) & equal, 0.0, -1e30)
        ones_back = [
            jnp.sum(
                jnp.where(equal & (key_pos == row_pos - by), 1.0, 0.0), axis=1, keepdims=True
            )
            for by in (1, 2)
        ]
        m_ref[...] = jnp.where(lane == 0, ones_back[0], ones_back[1])

        pairs = [(h, c) for h in range(kv_heads) for c in range(2)]
        upcoming = scores(*pairs[0])
        results = []
        for at in range(len(pairs)):
            score = upcoming
            if at + 1 < len(pairs):
                upcoming = scores(*pairs[at + 1])
            score = score.reshape(group, rows, keys) + bias[None]
            peak = jnp.max(score, axis=-1, keepdims=True)
            expd = jnp.exp2((score - peak) * mult).astype(jnp.bfloat16)
            both = jnp.dot(
                expd.reshape(group * rows, keys), v_ext, preferred_element_type=jnp.float32
            )
            results.append(both[:, :LANES] / both[:, LANES:])
        for h in range(kv_heads):
            here = (lane // head_width) == h
            outs = []
            for g in range(group):
                a = results[2 * h][g * rows : (g + 1) * rows]
                b = results[2 * h + 1][g * rows : (g + 1) * rows]
                o = jnp.where(here, a - lam_ref[h * group + g] * b, 0.0)
                meansq = jnp.sum(o * o, axis=-1, keepdims=True) * (1.0 / head_width)
                o = o * lax.rsqrt(meansq + NORM_EPS) * gain_row
                if (g % 2) != h:
                    o = pltpu.roll(o, head_width, 1)
                outs.append(o)
            for j in range(group // 2):
                tile = (h * group) // 2 + j
                h_ref[:, tile * LANES : (tile + 1) * LANES] = (
                    outs[2 * j] + outs[2 * j + 1]
                ).astype(jnp.bfloat16)
        o_ref[...] = jnp.dot(
            h_ref[...], p_ref[...], preferred_element_type=jnp.float32
        ).astype(jnp.bfloat16)

    smem = pl.BlockSpec(memory_space=pltpu.SMEM)
    vmem = pl.BlockSpec(memory_space=pltpu.VMEM)
    return pl.pallas_call(
        body,
        out_shape=(
            jax.ShapeDtypeStruct((rows, model), jnp.bfloat16),
            jax.ShapeDtypeStruct((rows, LANES), jnp.float32),
        ),
        in_specs=[smem, smem] + [vmem] * 8 + [pl.BlockSpec(memory_space=pl.ANY)],
        out_specs=(vmem, vmem),
        scratch_shapes=[pltpu.VMEM((rows, heads * head_width), jnp.bfloat16)],
        compiler_params=pltpu.CompilerParams(vmem_limit_bytes=24 * 1024 * 1024),
        cost_estimate=pl.CostEstimate(
            flops=3_000_000_000, transcendentals=0, bytes_accessed=4_000_000
        ),
        name="attend",
    )(place, lam, q_one, q_two, window, cosine, sine, docs, gain, out_weight, after)


def feed_forward(own, blocks, edges, same, weights, conv_gate, conv_value):
    rows, width = blocks[0].shape
    count = len(blocks)
    span = rows + EDGE
    total = span * count
    hidden = conv_gate.shape[1]
    step = 2 * LANES
    bounds = [0] + list(range(hidden % step, hidden + 1, step))
    cuts = list(zip(bounds[:-1], bounds[1:]))
    out_step = 16 * LANES

    def body(own_ref, *refs):
        x_in, e_in, m_in = refs[:count], refs[count : 2 * count], refs[2 * count : 3 * count]
        cg_ref, cv_ref, w_hbm = refs[3 * count : 3 * count + 3]
        o_ref, x_ref, w_ref, h_ref, b_ref, sems = refs[3 * count + 3 :]

        def piece(at, low, high, base, a, b):
            spot = (slice(low, high), slice(base + a, base + b))
            return pltpu.make_async_copy(w_hbm.at[spot], w_ref.at[spot], sems.at[at])

        queue = []
        for j, (a, b) in enumerate(cuts):
            queue.append([piece(2 * j + n, 0, width, n * hidden, a, b) for n in range(2)])
        for j in range(0, width, out_step):
            queue.append(
                [piece(2 * len(cuts) + j // out_step, j, j + out_step, 2 * hidden, 0, hidden)]
            )

        def launch(at):
            if at < len(queue):
                for copy in queue[at]:
                    copy.start()

        def arrive(at):
            for copy in queue[at]:
                copy.wait()
            launch(at + AHEAD)

        for at in range(AHEAD):
            launch(at)
        for k in range(count):
            x_ref[k * span : k * span + EDGE, :] = e_in[k][...]
            x_ref[k * span + EDGE : (k + 1) * span, :] = x_in[k][...]
            b_ref[k * span : k * span + EDGE, :] = jnp.zeros((EDGE, LANES), jnp.float32)
            b_ref[k * span + EDGE : (k + 1) * span, :] = m_in[k][...]
        one_back = b_ref[:, 0:1]
        two_back = b_ref[:, 1:2]

        def raised(j):
            a, b = cuts[j]
            arrive(j)
            return [
                jnp.dot(
                    x_ref[...], w_ref[:, base + a : base + b], preferred_element_type=jnp.float32
                ).astype(jnp.bfloat16)
                for base in (0, hidden)
            ]

        upcoming = raised(0)
        for j in range(len(cuts)):
            a, b = cuts[j]
            current = upcoming
            if j + 1 < len(cuts):
                upcoming = raised(j + 1)
            convs = []
            for u, taps in zip(current, (cg_ref, cv_ref)):
                u = u.astype(jnp.float32)
                convs.append(
                    taps[2:3, a:b] * u
                    + taps[1:2, a:b] * (one_back * pltpu.roll(u, 1, 0))
                    + taps[0:1, a:b] * (two_back * pltpu.roll(u, 2, 0))
                )
            g, v = convs
            act = g / (1.0 + jnp.exp(-g)) * v
            for k in range(count):
                h_ref[k * rows : (k + 1) * rows, a:b] = act[
                    k * span + EDGE : (k + 1) * span
                ].astype(jnp.bfloat16)
        for a in range(0, width, out_step):
            arrive(len(cuts) + a // out_step)
            part = lax.dot_general(
                h_ref[...],
                w_ref[a : a + out_step, 2 * hidden : 3 * hidden],
                (((1,), (1,)), ((), ())),
                preferred_element_type=jnp.float32,
            ).astype(jnp.bfloat16)
            for k in range(count):
                slot = (own_ref[0] - k + count) % count
                o_ref[slot, :, a : a + out_step] = part[k * rows : (k + 1) * rows]

    vmem = pl.BlockSpec(memory_space=pltpu.VMEM)
    return pl.pallas_call(
        body,
        out_shape=jax.ShapeDtypeStruct((count, rows, width), jnp.bfloat16),
        in_specs=[pl.BlockSpec(memory_space=pltpu.SMEM)] + [vmem] * (3 * count + 2) + [pl.BlockSpec(memory_space=pltpu.HBM)],
        out_specs=vmem,
        scratch_shapes=[
            pltpu.VMEM((total, width), jnp.bfloat16),
            pltpu.VMEM((width, 3 * hidden), jnp.bfloat16),
            pltpu.VMEM((count * rows, hidden), jnp.bfloat16),
            pltpu.VMEM((total, LANES), jnp.float32),
            pltpu.SemaphoreType.DMA((2 * len(cuts) + width // out_step,)),
        ],
        compiler_params=pltpu.CompilerParams(vmem_limit_bytes=48 * 1024 * 1024),
        name="feed_forward",
    )(own, *blocks, *edges, *same, conv_gate, conv_value, weights)


def per_device(
    resid_in,
    query_one,
    key_one,
    query_two,
    key_two,
    value,
    lam,
    head_gain,
    doc_ids,
    out_weight,
    norm_gain,
    gate_weight,
    value_weight,
    conv_gate,
    conv_value,
    down_weight,
):
    seqs, rows, q_lanes = query_one.shape
    width = q_lanes // lam.shape[0]
    rank = lax.axis_index("sp")
    ranks = lax.axis_size("sp")
    own = lax.axis_index("tp")
    parts = lax.axis_size("tp")
    model = resid_in.shape[2]

    packed = jnp.concatenate([gate_weight, value_weight, down_weight.T], axis=1)
    weights = lax.all_gather(packed, "sp", axis=0, tiled=True)

    positions = rank * rows + jnp.arange(rows, dtype=jnp.int32)
    cosine, sine = turn_tables(positions, width)
    keys = jnp.concatenate([key_one, key_two], axis=2).astype(jnp.float32)
    half = width // 2
    low = (jnp.arange(LANES) % width) < half
    swap = jnp.where(low, jnp.roll(keys, -half, axis=2), jnp.roll(keys, half, axis=2))
    keys = (keys * cosine + swap * sine).astype(jnp.bfloat16).astype(jnp.float32) * KEY_UP
    vals = value.astype(jnp.float32) * VAL_UP
    body_rows = jnp.concatenate([keys, vals], axis=2).reshape(seqs * rows, 2 * LANES)
    doc_rows = jnp.tile(doc_ids.astype(jnp.float32) * KEY_UP, (1, 2 * LANES // rows))
    doc_rows = jnp.pad(doc_rows, ((0, EDGE - seqs), (0, 0)))
    sent = jnp.concatenate([body_rows, doc_rows], axis=0).astype(jnp.float16)
    everyone = lax.all_gather(sent, "sp", axis=0, tiled=False)

    back = DOC_SPAN // rows
    span = min(back + 2, ranks)
    first = jnp.clip(rank // 2 * 2 - back, 0, ranks - span)
    lanes_down = jnp.where(jnp.arange(2 * LANES) < LANES, 1.0 / KEY_UP, 1.0 / VAL_UP)
    window = lax.dynamic_slice_in_dim(everyone, first, span, 0)
    window = (window.astype(jnp.float32) * lanes_down).astype(jnp.bfloat16)
    gain = head_gain.reshape(1, -1)
    proj = [None] * parts
    same = [None] * parts
    after = lam
    farthest_first = sorted(range(parts), key=lambda k: -min(k, parts - k))
    for k in farthest_first:
        place = jnp.stack([(own + k) % parts, first * rows, rank * rows]).astype(jnp.int32)
        proj[k], same[-k] = attend(
            place, query_one, query_two, window, cosine, sine, doc_ids, gain, lam, out_weight, after
        )
        after = proj[k]
    mid = resid_in[0].astype(jnp.float32) + proj[0].astype(jnp.float32)
    for k in range(1, parts):
        mid = mid + shifted(proj[k], "tp", k).astype(jnp.float32)
    meansq = jnp.mean(mid * mid, axis=-1, keepdims=True)
    normed = (mid * lax.rsqrt(meansq + NORM_EPS) * norm_gain).astype(jnp.bfloat16)
    edge = from_behind(normed[rows - EDGE :], "sp")
    blocks = [normed] + [shifted(normed, "tp", k) for k in range(1, parts)]
    edges = [edge] + [shifted(edge, "tp", k) for k in range(1, parts)]
    partial = feed_forward(
        own.reshape(1), blocks, edges, same, weights, conv_gate, conv_value
    )
    arrived = lax.all_to_all(partial, "tp", 0, 0, tiled=True)
    out = mid + jnp.sum(arrived.astype(jnp.float32), axis=0)
    return out.astype(jnp.bfloat16)[None]


def solution(mesh):
    placed = (
        P(("grp", "tp"), "sp", None),
        P("grp", "sp", "tp"),
        P("grp", "sp", "tp"),
        P("grp", "sp", "tp"),
        P("grp", "sp", "tp"),
        P("grp", "sp", "tp"),
        P("tp"),
        P(),
        P("grp", "sp"),
        P("tp", None),
        P(),
        P("sp", "tp"),
        P("sp", "tp"),
        P(None, "tp"),
        P(None, "tp"),
        P("tp", "sp"),
    )
    return jax.shard_map(
        per_device,
        mesh=mesh,
        in_specs=placed,
        out_specs=P(("grp", "tp"), "sp", None),
        check_vma=False,
    )
```

```python
import math

import jax
import jax.numpy as jnp
from jax import lax
from jax.experimental import pallas as pl
from jax.experimental.pallas import tpu as pltpu
from jax.sharding import PartitionSpec as P


NORM_EPS = 1e-06
ROPE_BASE = 500000.0
LOG2E = math.log2(math.e)
DOC_SPAN = 1024
KEY_UP = 4096.0
VAL_UP = 8192.0
LANES = 128
EDGE = 8
AHEAD = 3


def shifted(array, axis, by):
    length = lax.axis_size(axis)
    return lax.ppermute(array, axis, [(i, (i + by) % length) for i in range(length)])


def from_behind(array, axis):
    length = lax.axis_size(axis)
    return lax.ppermute(array, axis, [(i, i + 1) for i in range(length - 1)])


def turn_tables(positions, width):
    half = width // 2
    freqs = ROPE_BASE ** (-jnp.arange(half, dtype=jnp.float32) * 2.0 / width)
    angles = positions.astype(jnp.float32)[:, None] * freqs[None, :]
    cosine = jnp.cos(angles)
    sine = jnp.sin(angles)
    times = LANES // width
    return (
        jnp.tile(jnp.concatenate([cosine, cosine], axis=1), (1, times)),
        jnp.tile(jnp.concatenate([-sine, sine], axis=1), (1, times)),
    )


def attend(place, q_one, q_two, window, cosine, sine, docs, gain, lam, out_weight, after):
    seqs, rows, q_lanes = q_one.shape
    ranks, per_rank, _ = window.shape
    keys = ranks * rows
    heads = lam.shape[0]
    width = q_lanes // heads
    half = width // 2
    kv_heads = 2
    group = heads // kv_heads
    head_width = LANES // kv_heads
    mult = width ** (-0.5) * LOG2E
    model = out_weight.shape[1]

    def body(
        place_ref, lam_ref, q1_ref, q2_ref, w_ref, c_ref, s_ref, d_ref, g_ref, p_ref, _,
        o_ref, m_ref, h_ref,
    ):
        s = place_ref[0]
        first_key = place_ref[1]
        first_row = place_ref[2]
        lane = lax.broadcasted_iota(jnp.int32, (rows, LANES), 1)
        low = (lane % width) < half
        cos = c_ref[...]
        sin = s_ref[...]
        gain_row = jnp.concatenate([g_ref[...], g_ref[...]], axis=1)
        these = pl.ds(pl.multiple_of(s * rows, rows), rows)
        k_all = w_ref[:, these, 0:LANES].reshape(keys, LANES)
        v_all = w_ref[:, these, LANES : 2 * LANES].reshape(keys, LANES)
        v_ext = jnp.concatenate([v_all, jnp.ones((keys, LANES), jnp.bfloat16)], axis=1)

        placed = []
        for ref in (q1_ref, q2_ref):
            tiles = []
            for h in range(kv_heads):
                x = ref[s, :, h * LANES : (h + 1) * LANES].astype(jnp.float32)
                swap = jnp.where(low, pltpu.roll(x, LANES - half, 1), pltpu.roll(x, half, 1))
                tiles.append((x * cos + swap * sin).astype(jnp.bfloat16).astype(jnp.float32))
            placed.append(tiles)

        def scores(h, c):
            target = c * kv_heads + h
            inside = (lane // width) == target
            parts = []
            for g in range(group):
                by = (width * (target - g)) % LANES
                x = placed[c][h]
                x = pltpu.roll(x, by, 1) if by else x
                parts.append(jnp.where(inside, x, 0.0).astype(jnp.bfloat16))
            q = jnp.concatenate(parts, axis=0)
            return lax.dot_general(
                q, k_all, (((1,), (1,)), ((), ())), preferred_element_type=jnp.float32
            )

        key_pos = first_key + lax.broadcasted_iota(jnp.int32, (rows, keys), 1)
        row_pos = first_row + lax.broadcasted_iota(jnp.int32, (rows, keys), 0)
        even_lane = lax.broadcasted_iota(jnp.int32, (1, LANES), 1) < rows
        this_row = lax.broadcasted_iota(jnp.int32, (EDGE, LANES), 0) == s
        pieces = []
        for i in range(ranks // 2):
            two = [
                jnp.sum(
                    jnp.where(this_row, w_ref[2 * i + b, seqs * rows : per_rank, 0:LANES].astype(jnp.float32), 0.0),
                    axis=0,
                    keepdims=True,
                )
                for b in range(2)
            ]
            pieces.append(jnp.where(even_lane, two[0], two[1]))
        key_doc = jnp.concatenate(pieces, axis=1)
        diagonal = lax.broadcasted_iota(jnp.int32, (rows, rows), 0) == lax.broadcasted_iota(
            jnp.int32, (rows, rows), 1
        )
        row_doc = jnp.sum(
            jnp.where(diagonal, d_ref[pl.ds(s, 1), :].astype(jnp.float32), 0.0),
            axis=1,
            keepdims=True,
        )
        equal = key_doc == row_doc
        bias = jnp.where((key_pos <= row_pos) & equal, 0.0, -1e30)
        ones_back = [
            jnp.sum(
                jnp.where(equal & (key_pos == row_pos - by), 1.0, 0.0), axis=1, keepdims=True
            )
            for by in (1, 2)
        ]
        m_ref[...] = jnp.where(lane == 0, ones_back[0], ones_back[1])

        pairs = [(h, c) for h in range(kv_heads) for c in range(2)]
        upcoming = scores(*pairs[0])
        results = []
        for at in range(len(pairs)):
            score = upcoming
            if at + 1 < len(pairs):
                upcoming = scores(*pairs[at + 1])
            score = score.reshape(group, rows, keys) + bias[None]
            peak = jnp.max(score, axis=-1, keepdims=True)
            expd = jnp.exp2((score - peak) * mult).astype(jnp.bfloat16)
            both = jnp.dot(
                expd.reshape(group * rows, keys), v_ext, preferred_element_type=jnp.float32
            )
            results.append(both[:, :LANES] / both[:, LANES:])
        for h in range(kv_heads):
            here = (lane // head_width) == h
            outs = []
            for g in range(group):
                a = results[2 * h][g * rows : (g + 1) * rows]
                b = results[2 * h + 1][g * rows : (g + 1) * rows]
                o = jnp.where(here, a - lam_ref[h * group + g] * b, 0.0)
                meansq = jnp.sum(o * o, axis=-1, keepdims=True) * (1.0 / head_width)
                o = o * lax.rsqrt(meansq + NORM_EPS) * gain_row
                if (g % 2) != h:
                    o = pltpu.roll(o, head_width, 1)
                outs.append(o)
            for j in range(group // 2):
                tile = (h * group) // 2 + j
                h_ref[:, tile * LANES : (tile + 1) * LANES] = (
                    outs[2 * j] + outs[2 * j + 1]
                ).astype(jnp.bfloat16)
        o_ref[...] = jnp.dot(
            h_ref[...], p_ref[...], preferred_element_type=jnp.float32
        ).astype(jnp.bfloat16)

    smem = pl.BlockSpec(memory_space=pltpu.SMEM)
    vmem = pl.BlockSpec(memory_space=pltpu.VMEM)
    return pl.pallas_call(
        body,
        out_shape=(
            jax.ShapeDtypeStruct((rows, model), jnp.bfloat16),
            jax.ShapeDtypeStruct((rows, LANES), jnp.float32),
        ),
        in_specs=[smem, smem] + [vmem] * 8 + [pl.BlockSpec(memory_space=pl.ANY)],
        out_specs=(vmem, vmem),
        scratch_shapes=[pltpu.VMEM((rows, heads * head_width), jnp.bfloat16)],
        compiler_params=pltpu.CompilerParams(vmem_limit_bytes=24 * 1024 * 1024),
        cost_estimate=pl.CostEstimate(
            flops=3_000_000_000, transcendentals=0, bytes_accessed=4_000_000
        ),
        name="attend",
    )(place, lam, q_one, q_two, window, cosine, sine, docs, gain, out_weight, after)


def feed_forward(blocks, edges, same, weights, conv_gate, conv_value):
    rows, width = blocks[0].shape
    count = len(blocks)
    span = rows + EDGE
    total = span * count
    hidden = conv_gate.shape[1]
    step = 2 * LANES
    bounds = [0] + list(range(hidden % step, hidden + 1, step))
    cuts = list(zip(bounds[:-1], bounds[1:]))
    out_step = 16 * LANES

    def body(*refs):
        x_in, e_in, m_in = refs[:count], refs[count : 2 * count], refs[2 * count : 3 * count]
        cg_ref, cv_ref, w_hbm = refs[3 * count : 3 * count + 3]
        outs = refs[3 * count + 3 : 4 * count + 3]
        x_ref, w_ref, h_ref, b_ref, sems = refs[4 * count + 3 :]

        def piece(at, low, high, base, a, b):
            spot = (slice(low, high), slice(base + a, base + b))
            return pltpu.make_async_copy(w_hbm.at[spot], w_ref.at[spot], sems.at[at])

        queue = []
        for j, (a, b) in enumerate(cuts):
            queue.append([piece(2 * j + n, 0, width, n * hidden, a, b) for n in range(2)])
        for j in range(0, width, out_step):
            queue.append(
                [piece(2 * len(cuts) + j // out_step, j, j + out_step, 2 * hidden, 0, hidden)]
            )

        def launch(at):
            if at < len(queue):
                for copy in queue[at]:
                    copy.start()

        def arrive(at):
            for copy in queue[at]:
                copy.wait()
            launch(at + AHEAD)

        for at in range(AHEAD):
            launch(at)
        for k in range(count):
            x_ref[k * span : k * span + EDGE, :] = e_in[k][...]
            x_ref[k * span + EDGE : (k + 1) * span, :] = x_in[k][...]
            b_ref[k * span : k * span + EDGE, :] = jnp.zeros((EDGE, LANES), jnp.float32)
            b_ref[k * span + EDGE : (k + 1) * span, :] = m_in[k][...]
        one_back = b_ref[:, 0:1]
        two_back = b_ref[:, 1:2]

        def raised(j):
            a, b = cuts[j]
            arrive(j)
            return [
                jnp.dot(
                    x_ref[...], w_ref[:, base + a : base + b], preferred_element_type=jnp.float32
                ).astype(jnp.bfloat16)
                for base in (0, hidden)
            ]

        upcoming = raised(0)
        for j in range(len(cuts)):
            a, b = cuts[j]
            current = upcoming
            if j + 1 < len(cuts):
                upcoming = raised(j + 1)
            convs = []
            for u, taps in zip(current, (cg_ref, cv_ref)):
                u = u.astype(jnp.float32)
                convs.append(
                    taps[2:3, a:b] * u
                    + taps[1:2, a:b] * (one_back * pltpu.roll(u, 1, 0))
                    + taps[0:1, a:b] * (two_back * pltpu.roll(u, 2, 0))
                )
            g, v = convs
            act = g / (1.0 + jnp.exp(-g)) * v
            for k in range(count):
                h_ref[k * rows : (k + 1) * rows, a:b] = act[
                    k * span + EDGE : (k + 1) * span
                ].astype(jnp.bfloat16)
        for a in range(0, width, out_step):
            arrive(len(cuts) + a // out_step)
            part = lax.dot_general(
                h_ref[...],
                w_ref[a : a + out_step, 2 * hidden : 3 * hidden],
                (((1,), (1,)), ((), ())),
                preferred_element_type=jnp.float32,
            ).astype(jnp.bfloat16)
            for k in range(count):
                outs[k][:, a : a + out_step] = part[k * rows : (k + 1) * rows]

    vmem = pl.BlockSpec(memory_space=pltpu.VMEM)
    return pl.pallas_call(
        body,
        out_shape=[jax.ShapeDtypeStruct((rows, width), jnp.bfloat16)] * count,
        in_specs=[vmem] * (3 * count + 2) + [pl.BlockSpec(memory_space=pltpu.HBM)],
        out_specs=[vmem] * count,
        scratch_shapes=[
            pltpu.VMEM((total, width), jnp.bfloat16),
            pltpu.VMEM((width, 3 * hidden), jnp.bfloat16),
            pltpu.VMEM((count * rows, hidden), jnp.bfloat16),
            pltpu.VMEM((total, LANES), jnp.float32),
            pltpu.SemaphoreType.DMA((2 * len(cuts) + width // out_step,)),
        ],
        compiler_params=pltpu.CompilerParams(vmem_limit_bytes=48 * 1024 * 1024),
        name="feed_forward",
    )(*blocks, *edges, *same, conv_gate, conv_value, weights)


def per_device(
    resid_in,
    query_one,
    key_one,
    query_two,
    key_two,
    value,
    lam,
    head_gain,
    doc_ids,
    out_weight,
    norm_gain,
    gate_weight,
    value_weight,
    conv_gate,
    conv_value,
    down_weight,
):
    seqs, rows, q_lanes = query_one.shape
    width = q_lanes // lam.shape[0]
    rank = lax.axis_index("sp")
    ranks = lax.axis_size("sp")
    own = lax.axis_index("tp")
    parts = lax.axis_size("tp")

    packed = jnp.concatenate([gate_weight, value_weight, down_weight.T], axis=1)
    weights = lax.all_gather(packed, "sp", axis=0, tiled=True)

    positions = rank * rows + jnp.arange(rows, dtype=jnp.int32)
    cosine, sine = turn_tables(positions, width)
    keys = jnp.concatenate([key_one, key_two], axis=2).astype(jnp.float32)
    half = width // 2
    low = (jnp.arange(LANES) % width) < half
    swap = jnp.where(low, jnp.roll(keys, -half, axis=2), jnp.roll(keys, half, axis=2))
    keys = (keys * cosine + swap * sine).astype(jnp.bfloat16).astype(jnp.float32) * KEY_UP
    vals = value.astype(jnp.float32) * VAL_UP
    body_rows = jnp.concatenate([keys, vals], axis=2).reshape(seqs * rows, 2 * LANES)
    doc_rows = jnp.tile(doc_ids.astype(jnp.float32) * KEY_UP, (1, 2 * LANES // rows))
    doc_rows = jnp.pad(doc_rows, ((0, EDGE - seqs), (0, 0)))
    sent = jnp.concatenate([body_rows, doc_rows], axis=0).astype(jnp.float16)
    everyone = lax.all_gather(sent, "sp", axis=0, tiled=False)

    back = DOC_SPAN // rows
    span = min(back + 2, ranks)
    first = jnp.clip(rank // 2 * 2 - back, 0, ranks - span)
    lanes_down = jnp.where(jnp.arange(2 * LANES) < LANES, 1.0 / KEY_UP, 1.0 / VAL_UP)
    window = lax.dynamic_slice_in_dim(everyone, first, span, 0)
    window = (window.astype(jnp.float32) * lanes_down).astype(jnp.bfloat16)
    gain = head_gain.reshape(1, -1)
    proj = [None] * parts
    same = [None] * parts
    after = lam
    farthest_first = sorted(range(parts), key=lambda k: -min(k, parts - k))
    for k in farthest_first:
        place = jnp.stack([(own + k) % parts, first * rows, rank * rows]).astype(jnp.int32)
        proj[k], same[-k] = attend(
            place, query_one, query_two, window, cosine, sine, doc_ids, gain, lam, out_weight, after
        )
        after = proj[k]
    mid = resid_in[0].astype(jnp.float32) + proj[0].astype(jnp.float32)
    for k in range(1, parts):
        mid = mid + shifted(proj[k], "tp", k).astype(jnp.float32)
    meansq = jnp.mean(mid * mid, axis=-1, keepdims=True)
    normed = (mid * lax.rsqrt(meansq + NORM_EPS) * norm_gain).astype(jnp.bfloat16)
    edge = from_behind(normed[rows - EDGE :], "sp")
    blocks, edges = [normed] * parts, [edge] * parts
    for k in farthest_first[:-1]:
        blocks[k] = shifted(normed, "tp", k)
        edges[k] = shifted(edge, "tp", k)
    partial = feed_forward(blocks, edges, same, weights, conv_gate, conv_value)
    out = mid + partial[0].astype(jnp.float32)
    for k in farthest_first[:-1]:
        returned = shifted(partial[k], "tp", -k)
        out = out + returned.astype(jnp.float32)
    return out.astype(jnp.bfloat16)[None]


def solution(mesh):
    placed = (
        P(("grp", "tp"), "sp", None),
        P("grp", "sp", "tp"),
        P("grp", "sp", "tp"),
        P("grp", "sp", "tp"),
        P("grp", "sp", "tp"),
        P("grp", "sp", "tp"),
        P("tp"),
        P(),
        P("grp", "sp"),
        P("tp", None),
        P(),
        P("sp", "tp"),
        P("sp", "tp"),
        P(None, "tp"),
        P(None, "tp"),
        P("tp", "sp"),
    )

    return jax.shard_map(
        per_device,
        mesh=mesh,
        in_specs=placed,
        out_specs=P(("grp", "tp"), "sp", None),
        check_vma=False,
    )
```

```python
import math

import jax
import jax.numpy as jnp
from jax import lax
from jax.experimental import pallas as pl
from jax.experimental.pallas import tpu as pltpu
from jax.sharding import PartitionSpec as P


NORM_EPS = 1e-06
ROPE_BASE = 500000.0
LOG2E = math.log2(math.e)
DOC_SPAN = 1024
KEY_UP = 4096.0
VAL_UP = 8192.0
LANES = 128
EDGE = 8
AHEAD = 3


def shifted(array, axis, by):
    length = lax.axis_size(axis)
    return lax.ppermute(array, axis, [(i, (i + by) % length) for i in range(length)])


def from_behind(array, axis):
    length = lax.axis_size(axis)
    return lax.ppermute(array, axis, [(i, i + 1) for i in range(length - 1)])


def turn_tables(positions, width):
    half = width // 2
    freqs = ROPE_BASE ** (-jnp.arange(half, dtype=jnp.float32) * 2.0 / width)
    angles = positions.astype(jnp.float32)[:, None] * freqs[None, :]
    cosine = jnp.cos(angles)
    sine = jnp.sin(angles)
    times = LANES // width
    return (
        jnp.tile(jnp.concatenate([cosine, cosine], axis=1), (1, times)),
        jnp.tile(jnp.concatenate([-sine, sine], axis=1), (1, times)),
    )


def attend(place, q_one, q_two, window, cosine, sine, docs, gain, lam, out_weight, after):
    seqs, rows, q_lanes = q_one.shape
    ranks, per_rank, _ = window.shape
    keys = ranks * rows
    heads = lam.shape[0]
    width = q_lanes // heads
    half = width // 2
    kv_heads = 2
    group = heads // kv_heads
    head_width = LANES // kv_heads
    mult = width ** (-0.5) * LOG2E
    model = out_weight.shape[1]

    def body(
        place_ref, lam_ref, q1_ref, q2_ref, w_ref, c_ref, s_ref, d_ref, g_ref, p_ref, _,
        o_ref, m_ref, h_ref,
    ):
        s = place_ref[0]
        first_key = place_ref[1]
        first_row = place_ref[2]
        lane = lax.broadcasted_iota(jnp.int32, (rows, LANES), 1)
        low = (lane % width) < half
        cos = c_ref[...]
        sin = s_ref[...]
        gain_row = jnp.concatenate([g_ref[...], g_ref[...]], axis=1)
        these = pl.ds(pl.multiple_of(s * rows, rows), rows)
        k_all = w_ref[:, these, 0:LANES].reshape(keys, LANES)
        v_all = w_ref[:, these, LANES : 2 * LANES].reshape(keys, LANES)
        v_ext = jnp.concatenate([v_all, jnp.ones((keys, LANES), jnp.bfloat16)], axis=1)

        placed = []
        for ref in (q1_ref, q2_ref):
            tiles = []
            for h in range(kv_heads):
                x = ref[s, :, h * LANES : (h + 1) * LANES].astype(jnp.float32)
                swap = jnp.where(low, pltpu.roll(x, LANES - half, 1), pltpu.roll(x, half, 1))
                tiles.append((x * cos + swap * sin).astype(jnp.bfloat16).astype(jnp.float32))
            placed.append(tiles)

        def scores(h, c):
            target = c * kv_heads + h
            inside = (lane // width) == target
            parts = []
            for g in range(group):
                by = (width * (target - g)) % LANES
                x = placed[c][h]
                x = pltpu.roll(x, by, 1) if by else x
                parts.append(jnp.where(inside, x, 0.0).astype(jnp.bfloat16))
            q = jnp.concatenate(parts, axis=0)
            return lax.dot_general(
                q, k_all, (((1,), (1,)), ((), ())), preferred_element_type=jnp.float32
            )

        key_pos = first_key + lax.broadcasted_iota(jnp.int32, (rows, keys), 1)
        row_pos = first_row + lax.broadcasted_iota(jnp.int32, (rows, keys), 0)
        even_lane = lax.broadcasted_iota(jnp.int32, (1, LANES), 1) < rows
        this_row = lax.broadcasted_iota(jnp.int32, (EDGE, LANES), 0) == s
        pieces = []
        for i in range(ranks // 2):
            two = [
                jnp.sum(
                    jnp.where(this_row, w_ref[2 * i + b, seqs * rows : per_rank, 0:LANES].astype(jnp.float32), 0.0),
                    axis=0,
                    keepdims=True,
                )
                for b in range(2)
            ]
            pieces.append(jnp.where(even_lane, two[0], two[1]))
        key_doc = jnp.concatenate(pieces, axis=1)
        diagonal = lax.broadcasted_iota(jnp.int32, (rows, rows), 0) == lax.broadcasted_iota(
            jnp.int32, (rows, rows), 1
        )
        row_doc = jnp.sum(
            jnp.where(diagonal, d_ref[pl.ds(s, 1), :].astype(jnp.float32), 0.0),
            axis=1,
            keepdims=True,
        )
        equal = key_doc == row_doc
        bias = jnp.where((key_pos <= row_pos) & equal, 0.0, -1e30)
        ones_back = [
            jnp.sum(
                jnp.where(equal & (key_pos == row_pos - by), 1.0, 0.0), axis=1, keepdims=True
            )
            for by in (1, 2)
        ]
        m_ref[...] = jnp.where(lane == 0, ones_back[0], ones_back[1])

        pairs = [(h, c) for h in range(kv_heads) for c in range(2)]
        upcoming = scores(*pairs[0])
        results = []
        for at in range(len(pairs)):
            score = upcoming
            if at + 1 < len(pairs):
                upcoming = scores(*pairs[at + 1])
            score = score.reshape(group, rows, keys) + bias[None]
            peak = jnp.max(score, axis=-1, keepdims=True)
            expd = jnp.exp2((score - peak) * mult).astype(jnp.bfloat16)
            both = jnp.dot(
                expd.reshape(group * rows, keys), v_ext, preferred_element_type=jnp.float32
            )
            results.append(both[:, :LANES] / both[:, LANES:])
        for h in range(kv_heads):
            here = (lane // head_width) == h
            outs = []
            for g in range(group):
                a = results[2 * h][g * rows : (g + 1) * rows]
                b = results[2 * h + 1][g * rows : (g + 1) * rows]
                o = jnp.where(here, a - lam_ref[h * group + g] * b, 0.0)
                meansq = jnp.sum(o * o, axis=-1, keepdims=True) * (1.0 / head_width)
                o = o * lax.rsqrt(meansq + NORM_EPS) * gain_row
                if (g % 2) != h:
                    o = pltpu.roll(o, head_width, 1)
                outs.append(o)
            for j in range(group // 2):
                tile = (h * group) // 2 + j
                h_ref[:, tile * LANES : (tile + 1) * LANES] = (
                    outs[2 * j] + outs[2 * j + 1]
                ).astype(jnp.bfloat16)
        o_ref[...] = jnp.dot(
            h_ref[...], p_ref[...], preferred_element_type=jnp.float32
        ).astype(jnp.bfloat16)

    smem = pl.BlockSpec(memory_space=pltpu.SMEM)
    vmem = pl.BlockSpec(memory_space=pltpu.VMEM)
    return pl.pallas_call(
        body,
        out_shape=(
            jax.ShapeDtypeStruct((rows, model), jnp.bfloat16),
            jax.ShapeDtypeStruct((rows, LANES), jnp.float32),
        ),
        in_specs=[smem, smem] + [vmem] * 8 + [pl.BlockSpec(memory_space=pl.ANY)],
        out_specs=(vmem, vmem),
        scratch_shapes=[pltpu.VMEM((rows, heads * head_width), jnp.bfloat16)],
        compiler_params=pltpu.CompilerParams(vmem_limit_bytes=24 * 1024 * 1024),
        cost_estimate=pl.CostEstimate(
            flops=3_000_000_000, transcendentals=0, bytes_accessed=4_000_000
        ),
        name="attend",
    )(place, lam, q_one, q_two, window, cosine, sine, docs, gain, out_weight, after)


def feed_forward(blocks, edges, same, weights, conv_gate, conv_value):
    rows, width = blocks[0].shape
    count = len(blocks)
    span = rows + EDGE
    total = span * count
    hidden = conv_gate.shape[1]
    step = 2 * LANES
    bounds = [0] + list(range(hidden % step, hidden + 1, step))
    cuts = list(zip(bounds[:-1], bounds[1:]))
    out_step = 16 * LANES

    def body(*refs):
        x_in, e_in, m_in = refs[:count], refs[count : 2 * count], refs[2 * count : 3 * count]
        cg_ref, cv_ref, w_hbm = refs[3 * count : 3 * count + 3]
        outs = refs[3 * count + 3 : 4 * count + 3]
        x_ref, w_ref, h_ref, b_ref, sems = refs[4 * count + 3 :]

        def piece(at, low, high, base, a, b):
            spot = (slice(low, high), slice(base + a, base + b))
            return pltpu.make_async_copy(w_hbm.at[spot], w_ref.at[spot], sems.at[at])

        queue = []
        for j, (a, b) in enumerate(cuts):
            queue.append([piece(2 * j + n, 0, width, n * hidden, a, b) for n in range(2)])
        for j in range(0, width, out_step):
            queue.append(
                [piece(2 * len(cuts) + j // out_step, j, j + out_step, 2 * hidden, 0, hidden)]
            )

        def launch(at):
            if at < len(queue):
                for copy in queue[at]:
                    copy.start()

        def arrive(at):
            for copy in queue[at]:
                copy.wait()
            launch(at + AHEAD)

        for at in range(AHEAD):
            launch(at)
        for k in range(count):
            x_ref[k * span : k * span + EDGE, :] = e_in[k][...]
            x_ref[k * span + EDGE : (k + 1) * span, :] = x_in[k][...]
            b_ref[k * span : k * span + EDGE, :] = jnp.zeros((EDGE, LANES), jnp.float32)
            b_ref[k * span + EDGE : (k + 1) * span, :] = m_in[k][...]
        one_back = b_ref[:, 0:1]
        two_back = b_ref[:, 1:2]

        def raised(j):
            a, b = cuts[j]
            arrive(j)
            return [
                jnp.dot(
                    x_ref[...], w_ref[:, base + a : base + b], preferred_element_type=jnp.float32
                ).astype(jnp.bfloat16)
                for base in (0, hidden)
            ]

        upcoming = raised(0)
        for j in range(len(cuts)):
            a, b = cuts[j]
            current = upcoming
            if j + 1 < len(cuts):
                upcoming = raised(j + 1)
            convs = []
            for u, taps in zip(current, (cg_ref, cv_ref)):
                u = u.astype(jnp.float32)
                convs.append(
                    taps[2:3, a:b] * u
                    + taps[1:2, a:b] * (one_back * pltpu.roll(u, 1, 0))
                    + taps[0:1, a:b] * (two_back * pltpu.roll(u, 2, 0))
                )
            g, v = convs
            act = g / (1.0 + jnp.exp(-g)) * v
            for k in range(count):
                h_ref[k * rows : (k + 1) * rows, a:b] = act[
                    k * span + EDGE : (k + 1) * span
                ].astype(jnp.bfloat16)
        for a in range(0, width, out_step):
            arrive(len(cuts) + a // out_step)
            part = lax.dot_general(
                h_ref[...],
                w_ref[a : a + out_step, 2 * hidden : 3 * hidden],
                (((1,), (1,)), ((), ())),
                preferred_element_type=jnp.float32,
            ).astype(jnp.bfloat16)
            for k in range(count):
                outs[k][:, a : a + out_step] = part[k * rows : (k + 1) * rows]

    vmem = pl.BlockSpec(memory_space=pltpu.VMEM)
    return pl.pallas_call(
        body,
        out_shape=[jax.ShapeDtypeStruct((rows, width), jnp.bfloat16)] * count,
        in_specs=[vmem] * (3 * count + 2) + [pl.BlockSpec(memory_space=pltpu.HBM)],
        out_specs=[vmem] * count,
        scratch_shapes=[
            pltpu.VMEM((total, width), jnp.bfloat16),
            pltpu.VMEM((width, 3 * hidden), jnp.bfloat16),
            pltpu.VMEM((count * rows, hidden), jnp.bfloat16),
            pltpu.VMEM((total, LANES), jnp.float32),
            pltpu.SemaphoreType.DMA((2 * len(cuts) + width // out_step,)),
        ],
        compiler_params=pltpu.CompilerParams(vmem_limit_bytes=48 * 1024 * 1024),
        name="feed_forward",
    )(*blocks, *edges, *same, conv_gate, conv_value, weights)


def per_device(
    resid_in,
    query_one,
    key_one,
    query_two,
    key_two,
    value,
    lam,
    head_gain,
    doc_ids,
    out_weight,
    norm_gain,
    gate_weight,
    value_weight,
    conv_gate,
    conv_value,
    down_weight,
):
    seqs, rows, q_lanes = query_one.shape
    width = q_lanes // lam.shape[0]
    rank = lax.axis_index("sp")
    ranks = lax.axis_size("sp")
    own = lax.axis_index("tp")
    parts = lax.axis_size("tp")

    packed = jnp.concatenate([gate_weight, value_weight, down_weight.T], axis=1)
    weights = lax.all_gather(packed, "sp", axis=0, tiled=True)

    positions = rank * rows + jnp.arange(rows, dtype=jnp.int32)
    cosine, sine = turn_tables(positions, width)
    keys = jnp.concatenate([key_one, key_two], axis=2).astype(jnp.float32)
    half = width // 2
    low = (jnp.arange(LANES) % width) < half
    swap = jnp.where(low, jnp.roll(keys, -half, axis=2), jnp.roll(keys, half, axis=2))
    keys = (keys * cosine + swap * sine).astype(jnp.bfloat16).astype(jnp.float32) * KEY_UP
    vals = value.astype(jnp.float32) * VAL_UP
    body_rows = jnp.concatenate([keys, vals], axis=2).reshape(seqs * rows, 2 * LANES)
    doc_rows = jnp.tile(doc_ids.astype(jnp.float32) * KEY_UP, (1, 2 * LANES // rows))
    doc_rows = jnp.pad(doc_rows, ((0, EDGE - seqs), (0, 0)))
    sent = jnp.concatenate([body_rows, doc_rows], axis=0).astype(jnp.float16)
    everyone = lax.all_gather(sent, "sp", axis=0, tiled=False)

    back = DOC_SPAN // rows
    span = min(back + 2, ranks)
    first = jnp.clip(rank // 2 * 2 - back, 0, ranks - span)
    lanes_down = jnp.where(jnp.arange(2 * LANES) < LANES, 1.0 / KEY_UP, 1.0 / VAL_UP)
    window = lax.dynamic_slice_in_dim(everyone, first, span, 0)
    window = (window.astype(jnp.float32) * lanes_down).astype(jnp.bfloat16)
    gain = head_gain.reshape(1, -1)
    proj = [None] * parts
    same = [None] * parts
    after = lam
    farthest_first = sorted(range(parts), key=lambda k: -min(k, parts - k))
    for k in farthest_first:
        place = jnp.stack([(own + k) % parts, first * rows, rank * rows]).astype(jnp.int32)
        proj[k], same[-k] = attend(
            place, query_one, query_two, window, cosine, sine, doc_ids, gain, lam, out_weight, after
        )
        after = proj[k]
    mid = resid_in[0].astype(jnp.float32) + proj[0].astype(jnp.float32)
    for k in range(1, parts):
        mid = mid + shifted(proj[k], "tp", k).astype(jnp.float32)
    meansq = jnp.mean(mid * mid, axis=-1, keepdims=True)
    normed = (mid * lax.rsqrt(meansq + NORM_EPS) * norm_gain).astype(jnp.bfloat16)
    edge = from_behind(normed[rows - EDGE :], "sp")
    blocks = [normed] + [shifted(normed, "tp", k) for k in range(1, parts)]
    edges = [edge] + [shifted(edge, "tp", k) for k in range(1, parts)]
    partial = feed_forward(blocks, edges, same, weights, conv_gate, conv_value)
    out = mid + partial[0].astype(jnp.float32)
    for k in sorted(farthest_first[:-1], key=lambda k: (-min(k, parts - k), -k)):
        returned = shifted(partial[k], "tp", -k)
        out = out + returned.astype(jnp.float32)
    return out.astype(jnp.bfloat16)[None]


def solution(mesh):
    placed = (
        P(("grp", "tp"), "sp", None),
        P("grp", "sp", "tp"),
        P("grp", "sp", "tp"),
        P("grp", "sp", "tp"),
        P("grp", "sp", "tp"),
        P("grp", "sp", "tp"),
        P("tp"),
        P(),
        P("grp", "sp"),
        P("tp", None),
        P(),
        P("sp", "tp"),
        P("sp", "tp"),
        P(None, "tp"),
        P(None, "tp"),
        P("tp", "sp"),
    )

    return jax.shard_map(
        per_device,
        mesh=mesh,
        in_specs=placed,
        out_specs=P(("grp", "tp"), "sp", None),
        check_vma=False,
    )
```
